32 devices in a mesh: rep: 2 (over x), fs: 4 (over z), tp: 4 (over y, core).
Axes of the slice: x: 2, y: 2, z: 4, core: 2. Of those that a mesh axis runs over, the one named last changes fastest.
Arguments:
- tokens: bfloat16 [4096, 2048], P(('rep', 'fs', 'tp')), may hold values from -6 to 6
- mix_gain: float32 [2048], replicated, may hold values from 0.1 to 1.9
- w_query: bfloat16 [2048, 1024], P('fs', 'tp'), may hold values from -0.125 to 0.125
- w_key: bfloat16 [2048, 1024], P('fs', 'tp'), may hold values from -0.125 to 0.125
- w_value: bfloat16 [2048, 2048], P('fs', 'tp'), may hold values from -0.125 to 0.125
- w_decay_down: bfloat16 [2048, 32], replicated, may hold values from -0.125 to 0.125
- w_decay_up: bfloat16 [32, 1024], replicated, may hold values from -2 to 2
- decay_bias: float32 [1024], replicated, may hold values from -1 to 6
- decay_shift: float32 [4096, 1024], P(('rep', 'fs'), 'tp'), may hold values from -3 to 0
- head_gain: float32 [2048], replicated, may hold values from 0.1 to 1.9
- w_mix_out: bfloat16 [2048, 2048], P('tp', 'fs'), may hold values from -0.125 to 0.125
- ffn_gain: float32 [2048], replicated, may hold values from 0.1 to 1.9
- w_gate: bfloat16 [2048, 5632], P('fs', 'tp'), may hold values from -0.125 to 0.125
- w_up: bfloat16 [2048, 5632], P('fs', 'tp'), may hold values from -0.125 to 0.125
- w_down: bfloat16 [5632, 2048], P('tp', 'fs'), may hold values from -0.078125 to 0.078125
Outputs:
- layer_out: float32 [4096, 2048], P(('rep', 'fs', 'tp'))
The draws below stay inside these ranges and needn't reach their ends.
All inputs are finite; a program needn't handle non-finite values.
Results may differ from the reference program's by a relative error of at most 0.04.
Values may be sent and summed in bfloat16 or wider, within the bound.
A program may use at most 128 MiB of HBM per device.

```python
import jax
import jax.numpy as jnp
from jax import lax

D = 2048
HEADS = 8
KEY_CHANNELS = 128
DV = 256
KEY = 1024
RANK = 32
FF = 5632
BLK = 64
SEQUENCE_LENGTH = 512
TOKENS = 4096
N_TP = 4


def draw_decay_bias(key, part):
    head_key, fast_key, slow_key = jax.random.split(key, 3)
    fast_chance = 0.5
    fast_heads = jax.random.bernoulli(head_key, fast_chance, (HEADS,))
    fast_values = jax.random.uniform(fast_key, (HEADS, KEY_CHANNELS), jnp.float32, -0.5, 1.5)
    slow_values = jax.random.uniform(slow_key, (HEADS, KEY_CHANNELS), jnp.float32, 4.0, 6.0)
    return jnp.where(fast_heads[:, None], fast_values, slow_values).reshape(KEY).astype(jnp.float32)


def draw_decay_shift(key, part):
    sequence_count = TOKENS // SEQUENCE_LENGTH
    location_key, depth_key, rate_key = jax.random.split(key, 3)
    spike_locations = jax.random.randint(location_key, (sequence_count, 3), 0, SEQUENCE_LENGTH)
    spike_magnitudes = jnp.log(jax.random.uniform(depth_key, (sequence_count, 3, HEADS), jnp.float32, 0.5, 0.8))
    row_ids = jnp.arange(TOKENS)
    sequence_index = row_ids // SEQUENCE_LENGTH
    token_positions = row_ids % SEQUENCE_LENGTH
    match_flags = (token_positions[:, None] == spike_locations[sequence_index]).astype(jnp.float32)
    spike_events = jnp.einsum('fi,fit->ft', match_flags, spike_magnitudes[sequence_index])
    block_count = TOKENS // BLK
    rates = -jnp.exp(jax.random.uniform(rate_key, (block_count, KEY), jnp.float32, jnp.log(0.3), jnp.log(3.0))) / SEQUENCE_LENGTH
    decay_rate_rows = jnp.repeat(rates, BLK, axis=0)
    return (jnp.repeat(spike_events, KEY_CHANNELS, axis=1) + decay_rate_rows).astype(jnp.float32)


def shard_levels(stream_key, dims, cuts, smallest, top_value):
    level, own = 1.0, jax.random.fold_in(stream_key, 6)
    for position, parts in cuts:
        heights = jnp.exp(jax.random.uniform(jax.random.fold_in(own, position), (parts,), jnp.float32, smallest / len(cuts), top_value / len(cuts)))
        level = level * jnp.repeat(heights, dims[position] // parts).reshape([-1 if axis == position else 1 for axis in range(len(dims))])
    return level


def scatter_about(stream_key, shape, spread, bound, cuts=(), dtype=jnp.bfloat16):
    drawn = spread * jax.random.normal(stream_key, shape, jnp.float32)
    if cuts:
        drawn = drawn * shard_levels(stream_key, shape, cuts, -0.22, 0.18)
    return jnp.clip(drawn, -bound, bound).astype(dtype)


def setup_inputs(seed: int = 0) -> dict:
    streams_of = jax.random.split(jax.random.key(seed), 16)
    return {
        "tokens": scatter_about(streams_of[0], (TOKENS, D), 1.0, 6.0, ((0, 32),)),
        "mix_gain": jnp.clip(1.0 + 0.18 * jax.random.normal(streams_of[1], (D,), jnp.float32), 0.1, 1.9),
        "w_query": scatter_about(streams_of[2], (D, KEY), D ** -0.5, 0.125, ((0, 4), (1, 4))),
        "w_key": scatter_about(streams_of[3], (D, KEY), D ** -0.5, 0.125, ((0, 4), (1, 4))),
        "w_value": scatter_about(streams_of[4], (D, D), D ** -0.5, 0.125, ((0, 4), (1, 4))),
        "w_decay_down": scatter_about(streams_of[5], (D, RANK), D ** -0.5, 0.125),
        "w_decay_up": scatter_about(streams_of[6], (RANK, KEY), (RANK // 4) ** -0.5, 2.0),
        "decay_bias": draw_decay_bias(jax.random.fold_in(streams_of[15], 71), 0),
        "decay_shift": draw_decay_shift(jax.random.fold_in(streams_of[15], 71), 0),
        "head_gain": jnp.clip(1.0 + 0.18 * jax.random.normal(streams_of[9], (D,), jnp.float32), 0.1, 1.9),
        "w_mix_out": scatter_about(streams_of[10], (D, D), D ** -0.5, 0.125, ((0, 4), (1, 4))),
        "ffn_gain": jnp.clip(1.0 + 0.18 * jax.random.normal(streams_of[11], (D,), jnp.float32), 0.1, 1.9),
        "w_gate": scatter_about(streams_of[12], (D, FF), D ** -0.5, 0.125, ((0, 4), (1, 4))),
        "w_up": scatter_about(streams_of[13], (D, FF), D ** -0.5, 0.125, ((0, 4), (1, 4))),
        "w_down": scatter_about(streams_of[14], (FF, D), FF ** -0.5, 0.078125, ((0, 4), (1, 4))),
    }


EPS = 1e-06
TAU = 16.0

def rms_norm(values, gain):
    return values * lax.rsqrt(lax.optimization_barrier(jnp.mean(values * values, axis=-1, keepdims=True)) + EPS) * gain

def recurrence(query_proj, key_proj, value_proj, log_decay):
    blocks = SEQUENCE_LENGTH // BLK
    queries = query_proj.astype(jnp.float32).reshape(blocks, BLK, HEADS, KEY_CHANNELS) * KEY_CHANNELS ** (-0.5)
    keys = key_proj.astype(jnp.float32).reshape(blocks, BLK, HEADS, KEY_CHANNELS)
    values = value_proj.astype(jnp.float32).reshape(blocks, BLK, HEADS, DV)
    decays = log_decay.reshape(blocks, BLK, HEADS, KEY_CHANNELS)
    cumul = jnp.cumsum(decays, axis=1)
    totals = cumul[:, -1]
    weighted = keys * jnp.exp(totals[:, None] - cumul)
    updates = jnp.einsum('bchd,bche->bhde', weighted, values, precision=lax.Precision.HIGHEST)

    def advance(state, inputs):
        total, update = inputs
        new_state = jnp.exp(total)[..., None] * state + update
        return (new_state, state)
    _, previous = lax.scan(advance, jnp.zeros((HEADS, KEY_CHANNELS, DV), jnp.float32), (totals, updates))
    q_decayed = queries * jnp.exp(cumul)
    k_decayed = keys * jnp.exp(-cumul)
    scores = jnp.einsum('bchd,bshd->bhcs', q_decayed, k_decayed, precision=lax.Precision.HIGHEST)
    causal = (jnp.arange(BLK)[:, None] >= jnp.arange(BLK)[None, :]).astype(jnp.float32)
    scores = scores * causal
    inner = jnp.einsum('bhcs,bshe->bche', scores, values, precision=lax.Precision.HIGHEST)
    carried = jnp.einsum('bchd,bhde->bche', q_decayed, previous, precision=lax.Precision.HIGHEST)
    return (inner + carried).reshape(SEQUENCE_LENGTH, HEADS, DV)

def reference(tokens, mix_gain, w_query, w_key, w_value, w_decay_down, w_decay_up, decay_bias, decay_shift, head_gain, w_mix_out, ffn_gain, w_gate, w_up, w_down):
    sequence_count = TOKENS // SEQUENCE_LENGTH
    out_groups = w_mix_out.astype(jnp.float32).reshape(N_TP, D // N_TP, D)
    down_groups = w_down.astype(jnp.float32).reshape(N_TP, FF // N_TP, D)

    def layer(inputs):
        seq_tokens, seq_shift = inputs
        source = seq_tokens.astype(jnp.float32)
        normed = rms_norm(source, mix_gain).astype(jnp.bfloat16)
        query_proj = jnp.dot(normed, w_query, preferred_element_type=jnp.float32).astype(jnp.bfloat16)
        key_proj = jnp.dot(normed, w_key, preferred_element_type=jnp.float32).astype(jnp.bfloat16)
        value_proj = jnp.dot(normed, w_value, preferred_element_type=jnp.float32).astype(jnp.bfloat16)
        low_rank = jnp.dot(normed, w_decay_down, preferred_element_type=jnp.float32).astype(jnp.bfloat16)
        pre_decay = jnp.dot(low_rank, w_decay_up, preferred_element_type=jnp.float32) + decay_bias
        log_decay = jax.nn.log_sigmoid(pre_decay) / TAU + seq_shift
        head_out = recurrence(query_proj, key_proj, value_proj, log_decay)
        gated = rms_norm(head_out, head_gain.reshape(HEADS, DV)).astype(jnp.bfloat16)
        gated = gated.reshape(SEQUENCE_LENGTH, N_TP, D // N_TP).astype(jnp.float32)
        partials = jnp.einsum('lgc,gcd->gld', gated, out_groups).astype(jnp.bfloat16)
        hidden = source + lax.optimization_barrier(jnp.sum(partials.astype(jnp.float32), axis=0))
        normed_ffn = rms_norm(hidden, ffn_gain).astype(jnp.bfloat16)
        gate_proj = jnp.dot(normed_ffn, w_gate, preferred_element_type=jnp.float32)
        up_proj = jnp.dot(normed_ffn, w_up, preferred_element_type=jnp.float32)
        activated = (jax.nn.silu(gate_proj) * up_proj).astype(jnp.bfloat16)
        activated = activated.reshape(SEQUENCE_LENGTH, N_TP, FF // N_TP).astype(jnp.float32)
        ffn_parts = jnp.einsum('lgc,gcd->gld', activated, down_groups).astype(jnp.bfloat16)
        return hidden + lax.optimization_barrier(jnp.sum(ffn_parts.astype(jnp.float32), axis=0))
    result = lax.map(layer, (tokens.reshape(sequence_count, SEQUENCE_LENGTH, D), decay_shift.reshape(sequence_count, SEQUENCE_LENGTH, KEY)))
    return result.reshape(TOKENS, D)
```

```python
import jax
import jax.numpy as jnp
from jax import lax
from jax.experimental import pallas as pl
from jax.experimental.pallas import tpu as pltpu
from jax.sharding import PartitionSpec as P

KEY_CHANNELS = 128
DV = 256
BLK = 64


EPS = 1e-06
TAU = 16.0


def rms_norm(values, gain):
    return values * lax.rsqrt(jnp.mean(values * values, axis=-1, keepdims=True) + EPS) * gain


def recurrence(query_proj, key_proj, value_proj, log_decay, head_count):
    seq_rows = query_proj.shape[0]
    blocks = seq_rows // BLK
    exact = lax.Precision.HIGHEST
    queries = query_proj.astype(jnp.float32).reshape(
        blocks, BLK, head_count, KEY_CHANNELS
    ) * KEY_CHANNELS ** (-0.5)
    keys = key_proj.astype(jnp.float32).reshape(blocks, BLK, head_count, KEY_CHANNELS)
    values = value_proj.astype(jnp.float32).reshape(blocks, BLK, head_count, DV)
    decays = log_decay.reshape(blocks, BLK, head_count, KEY_CHANNELS)
    lower = (jnp.arange(BLK)[:, None] >= jnp.arange(BLK)[None, :]).astype(jnp.float32)
    cumul = jnp.einsum("cs,bshd->bchd", lower, decays, precision=exact)
    totals = cumul[:, -1]
    weighted = keys * jnp.exp(totals[:, None] - cumul)
    updates = jnp.einsum("bchd,bche->bhde", weighted, values, precision=exact)
    state = jnp.zeros_like(updates[0])
    previous = []
    for block in range(blocks):
        previous.append(state)
        state = jnp.exp(totals[block])[..., None] * state + updates[block]
    previous = jnp.stack(previous)
    q_decayed = queries * jnp.exp(cumul)
    k_decayed = keys * jnp.exp(-cumul)
    scores = jnp.einsum("bchd,bshd->bhcs", q_decayed, k_decayed, precision=exact)
    scores = scores * lower
    inner = jnp.einsum("bhcs,bshe->bche", scores, values, precision=exact)
    carried = jnp.einsum("bchd,bhde->bche", q_decayed, previous, precision=exact)
    return (inner + carried).reshape(seq_rows, head_count, DV)


def shift(values, axis, distance):
    count = lax.axis_size(axis)
    return lax.ppermute(values, axis, [(i, (i + distance) % count) for i in range(count)])


def swap_core(values):
    return lax.ppermute(values, "tp", [(i, i ^ 1) for i in range(lax.axis_size("tp"))])


def gather_rows(block):
    count = lax.axis_size("tp")
    index = lax.axis_index("tp")
    chips, core, chip = count // 2, index % 2, index // 2
    rows = block.shape[0]
    mine = [block] + [shift(block, "tp", 2 * k) for k in range(1, chips)]
    whole = jnp.zeros((count * rows,) + block.shape[1:], block.dtype)
    for k, piece in enumerate(mine):
        source = (chip - k) % chips
        theirs = swap_core(piece)
        whole = lax.dynamic_update_slice_in_dim(whole, piece, (2 * source + core) * rows, 0)
        whole = lax.dynamic_update_slice_in_dim(whole, theirs, (2 * source + 1 - core) * rows, 0)
    return whole


def scatter_sum(partial):
    count = lax.axis_size("tp")
    index = lax.axis_index("tp")
    chips, core, chip = count // 2, index % 2, index // 2
    rows = partial.shape[0] // count
    blocks = partial.astype(jnp.bfloat16).reshape(chips, 2, rows, partial.shape[1])
    away = lax.dynamic_index_in_dim(blocks, 1 - core, 1, keepdims=False)
    kept = lax.dynamic_index_in_dim(blocks, core, 1, keepdims=False).astype(jnp.float32)
    pair = kept + swap_core(away).astype(jnp.float32)
    rounded = pair.astype(jnp.bfloat16)
    total = lax.dynamic_index_in_dim(pair, chip, 0, keepdims=False)
    for k in range(1, chips):
        outgoing = lax.dynamic_index_in_dim(rounded, (chip + k) % chips, 0, keepdims=False)
        total = total + shift(outgoing, "tp", 2 * k).astype(jnp.float32)
    return total


def row_parts(weight):
    reps = lax.axis_size("rep")
    share = weight.shape[0] // reps
    own = lax.dynamic_slice_in_dim(weight, lax.axis_index("rep") * share, share, 0)
    own = lax.all_gather(own, "fs", axis=0, tiled=True)
    return [own] + [shift(own, "rep", k) for k in range(1, reps)]


def column_parts(weight):
    reps = lax.axis_size("rep")
    share = weight.shape[1] // reps
    own = lax.dynamic_slice_in_dim(weight, lax.axis_index("rep") * share, share, 1)
    own = lax.all_gather(own, "fs", axis=0, tiled=False)
    return [own] + [shift(own, "rep", k) for k in range(1, reps)]


def input_parts(values):
    reps, groups = lax.axis_size("rep"), lax.axis_size("fs")
    share = values.shape[1] // (reps * groups)
    layouts = [
        jnp.concatenate(
            [
                values[:, (g * reps + j) * share : (g * reps + j + 1) * share]
                for g in range(groups)
            ],
            axis=1,
        )
        for j in range(reps)
    ]
    index = lax.axis_index("rep")
    return [
        lax.select_n(jnp.full((), (index - k) % reps, jnp.int32), *layouts) if reps > 2
        else (jnp.where((index - k) % reps == 0, layouts[0], layouts[-1]))
        for k in range(reps)
    ]


def dots(inputs, weights):
    total = jnp.dot(inputs[0], weights[0], preferred_element_type=jnp.float32)
    for left, right in zip(inputs[1:], weights[1:]):
        total = total + jnp.dot(left, right, preferred_element_type=jnp.float32)
    return total


def project_out(values, weights):
    reps = lax.axis_size("rep")
    index = lax.axis_index("rep")
    sums = []
    for weight in weights:
        partial = jnp.concatenate(
            [
                jnp.dot(values, weight[g], preferred_element_type=jnp.float32)
                for g in range(weight.shape[0])
            ],
            axis=1,
        )
        sums.append(scatter_sum(partial))
    share = weights[0].shape[2]
    ordered = []
    for j in range(reps):
        if reps == 2:
            ordered.append(jnp.where(index == j, sums[0], sums[1]))
        else:
            ordered.append(lax.select_n((index - j) % reps, *sums))
    pieces = []
    for g in range(weights[0].shape[0]):
        for j in range(reps):
            pieces.append(ordered[j][:, g * share : (g + 1) * share])
    return jnp.concatenate(pieces, axis=1)


def per_device(
    tokens,
    mix_gain,
    w_query,
    w_key,
    w_value,
    w_decay_down,
    w_decay_up,
    decay_bias,
    decay_shift,
    head_gain,
    w_mix_out,
    ffn_gain,
    w_gate,
    w_up,
    w_down,
):
    tp_index = lax.axis_index("tp")
    key_cols = w_query.shape[1]
    value_cols = w_value.shape[1]
    heads_dev = key_cols // KEY_CHANNELS
    own_tokens = tokens.astype(jnp.float32)
    qkv_weights = row_parts(jnp.concatenate([w_query, w_key, w_value], axis=1))
    out_weights = column_parts(w_mix_out)
    gate_weights = row_parts(w_gate)
    up_weights = row_parts(w_up)
    down_weights = column_parts(w_down)
    normed = gather_rows(rms_norm(own_tokens, mix_gain).astype(jnp.bfloat16))
    seq_rows = normed.shape[0]
    low_rank = jnp.dot(normed, w_decay_down, preferred_element_type=jnp.float32).astype(
        jnp.bfloat16
    )
    up_columns = lax.dynamic_slice_in_dim(w_decay_up, tp_index * key_cols, key_cols, 1)
    bias_columns = lax.dynamic_slice_in_dim(decay_bias, tp_index * key_cols, key_cols, 0)
    pre_decay = jnp.dot(low_rank, up_columns, preferred_element_type=jnp.float32) + bias_columns
    log_decay = jax.nn.log_sigmoid(pre_decay) / TAU + decay_shift
    projected = dots(input_parts(normed), qkv_weights).astype(jnp.bfloat16)
    query_proj = projected[:, :key_cols]
    key_proj = projected[:, key_cols : 2 * key_cols]
    value_proj = projected[:, 2 * key_cols :]
    head_out = recurrence(query_proj, key_proj, value_proj, log_decay, heads_dev)
    gain_columns = lax.dynamic_slice_in_dim(head_gain, tp_index * value_cols, value_cols, 0)
    gated = rms_norm(head_out, gain_columns.reshape(heads_dev, DV)).astype(jnp.bfloat16)
    gated = gated.reshape(seq_rows, value_cols)
    hidden = own_tokens + project_out(gated, out_weights)
    normed_ffn = gather_rows(rms_norm(hidden, ffn_gain).astype(jnp.bfloat16))
    ffn_inputs = input_parts(normed_ffn)
    gate_proj = dots(ffn_inputs, gate_weights)
    up_proj = dots(ffn_inputs, up_weights)
    activated = (jax.nn.silu(gate_proj) * up_proj).astype(jnp.bfloat16)
    return hidden + project_out(activated, down_weights)


BF16 = jnp.bfloat16
F32 = jnp.float32
MESH_ID = pl.DeviceIdType.MESH
KINDS = ("end_a", "end_b", "mid_own", "mid_end", "rep_own", "rep_end")
PARTS = ("qkv", "out", "gate0", "up0", "gate1", "up1", "down")


def layer_kernel(
    tokens, mix_gain, w_query, w_key, w_value, w_decay_down, w_decay_up, decay_bias,
    decay_shift, head_gain, w_mix_out, ffn_gain, w_gate, w_up, w_down,
    out,
    wq, wo, wg, wu, wd, tok, shift, x_mix, x_ffn, proj, gated, part, near, far, near2, far2,
    act, hid, mixed_home, ffn_home, state,
    load_sem, w_send, w_recv, a_send, a_recv,
):
    r, z, t = lax.axis_index("rep"), lax.axis_index("fs"), lax.axis_index("tp")
    depth, key_cols = w_query.shape
    value_cols = w_value.shape[1]
    rows, width = tokens.shape
    seq = rows * 4
    hidden_units = w_gate.shape[1]
    block = width // 8
    half_rows = depth // 2
    cut = (hidden_units // 256 + 1) // 2 * 256
    heads = key_cols // KEY_CHANNELS
    zc = 1 + z // 2
    ze = 3 * (z // 2)
    zo, zf = 3 - zc, 3 - ze
    other_r = 1 - r
    core = t + 1 - 2 * lax.rem(t, 2)
    chip = lax.rem(t + 2, 4)
    both = 3 - t
    pair_z = z + 1 - 2 * lax.rem(z, 2)
    is_centre = jnp.logical_and(z >= 1, z <= 2)

    barrier = pltpu.get_barrier_semaphore()
    for partner in ({"fs": pair_z}, {"fs": 3 - z}, {"rep": other_r}, {"tp": core}, {"tp": chip}):
        pl.semaphore_signal(barrier, inc=1, device_id=partner, device_id_type=MESH_ID)

    def region(name, plane, half):
        at = pl.multiple_of(plane * depth + half * half_rows, half_rows)
        if name == "qkv":
            return wq.at[pl.ds(at, half_rows), :]
        if name == "out":
            return wo.at[2 * plane + half]
        if name == "down":
            return wd.at[2 * plane + half]
        ref = wg if name.startswith("gate") else wu
        if name.endswith("0"):
            return ref.at[pl.ds(at, half_rows), pl.ds(0, cut)]
        return ref.at[pl.ds(at, half_rows), pl.ds(cut, hidden_units - cut)]

    def weight_copy(name, kind, plane, half, device):
        ref = region(name, plane, half)
        index = PARTS.index(name) * len(KINDS) + KINDS.index(kind)
        return pltpu.make_async_remote_copy(
            src_ref=ref, dst_ref=ref, send_sem=w_send.at[index], recv_sem=w_recv.at[index],
            device_id=device, device_id_type=MESH_ID,
        )

    names = iter(range(1000))
    act_ids = {}

    def act_copy(key, src, dst, device):
        index = act_ids.setdefault(key, len(act_ids))
        return pltpu.make_async_remote_copy(
            src_ref=src, dst_ref=dst, send_sem=a_send.at[index], recv_sem=a_recv.at[index],
            device_id=device, device_id_type=MESH_ID,
        )

    at_z = pl.multiple_of(z * depth, depth)
    loads = {}

    def load(name, src, dst):
        copy = pltpu.make_async_copy(src, dst, load_sem.at[len(loads)])
        copy.start()
        loads[name] = copy

    load("q", w_query, wq.at[pl.ds(at_z, depth), pl.ds(0, key_cols)])
    load("k", w_key, wq.at[pl.ds(at_z, depth), pl.ds(key_cols, key_cols)])
    load("v", w_value, wq.at[pl.ds(at_z, depth), pl.ds(2 * key_cols, value_cols)])
    load("tok", tokens, tok.at[0])
    load("o0", w_mix_out.at[:, pl.ds(0, block)], wo.at[2 * z])
    load("o1", w_mix_out.at[:, pl.ds(block, block)], wo.at[2 * z + 1])
    load("shift", decay_shift, shift.at[0])
    load("g", w_gate, wg.at[pl.ds(at_z, depth), :])
    load("u", w_up, wu.at[pl.ds(at_z, depth), :])
    load("d0", w_down.at[:, pl.ds(0, block)], wd.at[2 * z])
    load("d1", w_down.at[:, pl.ds(block, block)], wd.at[2 * z + 1])
    pl.semaphore_wait(barrier, 5)
    for name in ("q", "k", "v"):
        loads[name].wait()

    tok_copy = act_copy("tok", tok.at[0], tok.at[1], {"fs": pair_z})
    shift_copy = act_copy("shift", shift.at[0], shift.at[1], {"fs": pair_z})

    out_order = [
        (2 * zc, None), (2 * zc + 1, None),
        (2 * zo + r, ("mid_own", zo, r)), (2 * ze + r, ("end_a", ze, r)),
        (2 * zo + other_r, ("rep_own", zo, other_r)), (2 * zf + r, ("mid_end", zf, r)),
        (2 * ze + other_r, ("end_b", ze, other_r)), (2 * zf + other_r, ("rep_end", zf, other_r)),
    ]
    mixed_copy = act_copy("mixed", mixed_home, mixed_home, {"fs": pair_z})
    home_copies = [
        act_copy(("home", i), ffn_home.at[b], ffn_home.at[b], {"fs": pair_z})
        for i, (b, _) in enumerate(out_order)
    ]

    @pl.when(jnp.logical_not(is_centre))
    def _():
        sent = []

        def send(name, kind, half):
            copy = weight_copy(name, kind, z, half, {"fs": pair_z})
            copy.start()
            sent.append(copy)

        send("qkv", "end_a", r)
        loads["tok"].wait()
        tok_copy.start()
        loads["o0"].wait()
        loads["o1"].wait()
        send("out", "end_a", r)
        send("qkv", "end_b", other_r)
        loads["shift"].wait()
        shift_copy.start()
        loads["g"].wait()
        loads["u"].wait()
        send("gate0", "end_a", r)
        send("up0", "end_a", r)
        send("out", "end_b", other_r)
        send("gate0", "end_b", other_r)
        send("up0", "end_b", other_r)
        send("gate1", "end_a", r)
        send("up1", "end_a", r)
        loads["d0"].wait()
        loads["d1"].wait()
        send("down", "end_a", r)
        send("gate1", "end_b", other_r)
        send("up1", "end_b", other_r)
        send("down", "end_b", other_r)
        mixed_copy.wait_recv()
        for i, (b, _) in enumerate(out_order):
            home_copies[i].wait_recv()
            cols = pl.ds(pl.multiple_of(b * block, block), block)
            out[:, cols] = (
                tok[0, :, cols].astype(F32) + mixed_home[b].astype(F32) + ffn_home[b].astype(F32)
            )
        tok_copy.wait_send()
        shift_copy.wait_send()
        for copy in sent:
            copy.wait_send()

    @pl.when(is_centre)
    def _():
        sent = []

        def incoming(name, kind, plane, half):
            weight_copy(name, kind, plane, half, {"fs": pair_z}).wait_recv()

        def send(name, kind, plane, half, device):
            copy = weight_copy(name, kind, plane, half, device)
            copy.start()
            sent.append(copy)

        def mid_own(*parts):
            for name in parts:
                send(name, "mid_own", z, r, {"fs": zo})

        def mid_end(*parts):
            for name in parts:
                incoming(name, "end_a", ze, r)
                send(name, "mid_end", ze, r, {"fs": zo})

        def rep_own(*parts):
            for name in parts:
                incoming(name, "mid_own", zo, r)
                send(name, "rep_own", zo, r, {"rep": other_r})

        def rep_end(*parts):
            for name in parts:
                incoming(name, "mid_end", zf, r)
                send(name, "rep_end", zf, r, {"rep": other_r})

        def complete(*parts):
            for name in parts:
                incoming(name, "end_b", ze, other_r)
                incoming(name, "rep_own", zo, other_r)
                incoming(name, "rep_end", zf, other_r)

        def norm_rows(load_rows, gain, dst, s):
            @pl.loop(0, rows // 16)
            def _(i):
                values = load_rows(pl.ds(pl.multiple_of(i * 16, 16), 16))
                scale = lax.rsqrt(jnp.mean(values * values, axis=-1, keepdims=True) + EPS)
                at = pl.multiple_of(t * rows + i * 16, 16)
                dst[s, pl.ds(at, 16), :] = (values * scale * gain[...]).astype(BF16)

        class Gather:
            def __init__(self, key, ref, s):
                def rows_of(device):
                    return ref.at[s, pl.ds(pl.multiple_of(device * rows, rows), rows), :]

                mine, theirs = rows_of(t), rows_of(chip)
                self.to_chip = act_copy((key, s, "chip"), mine, mine, {"tp": chip})
                self.to_core = act_copy((key, s, "core"), mine, mine, {"tp": core})
                self.pass_on = act_copy((key, s, "pass"), theirs, theirs, {"tp": core})
                self.from_chip = act_copy((key, s, "chip"), theirs, theirs, {"tp": chip})
                self.from_core = act_copy((key, s, "core"), rows_of(core), rows_of(core), {"tp": core})
                self.passed = act_copy((key, s, "pass"), rows_of(both), rows_of(both), {"tp": core})

            def start(self):
                self.to_chip.start()
                self.to_core.start()

            def forward(self):
                self.from_chip.wait_recv()
                self.pass_on.start()

            def finish(self):
                self.from_core.wait_recv()
                self.passed.wait_recv()

            def drain(self):
                self.to_chip.wait_send()
                self.to_core.wait_send()
                self.pass_on.wait_send()

        mid_own("qkv")
        loads["o0"].wait()
        loads["o1"].wait()
        mid_own("out")
        loads["tok"].wait()
        norm_rows(lambda at: tok[0, at, :].astype(F32), mix_gain, x_mix, 0)
        mix_gather = [Gather("mix", x_mix, s) for s in range(2)]
        ffn_gather = [Gather("ffn", x_ffn, s) for s in range(2)]
        mix_gather[0].start()
        loads["shift"].wait()
        loads["g"].wait()
        loads["u"].wait()
        mid_end("qkv")
        rep_own("qkv")
        mix_gather[0].forward()
        mid_own("gate0", "up0")
        tok_copy.wait_recv()
        norm_rows(lambda at: tok[1, at, :].astype(F32), mix_gain, x_mix, 1)
        mix_gather[1].start()
        rep_end("qkv")
        mid_end("out")
        rep_own("out")
        mid_own("gate1", "up1")
        mix_gather[1].forward()
        loads["d0"].wait()
        loads["d1"].wait()
        mix_gather[0].finish()
        mix_gather[1].finish()
        complete("qkv")

        bias = decay_bias[:, pl.ds(pl.multiple_of(t * key_cols, key_cols), key_cols)]
        up_cols = w_decay_up[:, pl.ds(pl.multiple_of(t * key_cols, key_cols), key_cols)]

        def project(s):
            @pl.loop(0, seq // 256)
            def _(i):
                at = pl.ds(pl.multiple_of(i * 256, 256), 256)
                x = x_mix[s, at, :]
                for n in range(0, 2 * key_cols + value_cols, 512):
                    cols = pl.ds(n, 512)
                    proj[s, at, cols] = jnp.dot(x, wq[:, cols], preferred_element_type=F32).astype(BF16)
                low = jnp.dot(x, w_decay_down[...], preferred_element_type=F32).astype(BF16)
                pre = jnp.dot(low, up_cols, preferred_element_type=F32) + bias
                log_sig = jnp.minimum(pre, 0.0) - jnp.log1p(jnp.exp(-jnp.abs(pre)))
                shift[s, at, :] = log_sig / TAU + shift[s, at, :]

        lower = (
            lax.broadcasted_iota(jnp.int32, (BLK, BLK), 0) >= lax.broadcasted_iota(jnp.int32, (BLK, BLK), 1)
        )
        gain_cols = head_gain[:, pl.ds(pl.multiple_of(t * value_cols, value_cols), value_cols)]

        def attend(s):
            state[...] = jnp.zeros_like(state)

            @pl.loop(0, seq // BLK)
            def _(b):
                at = pl.ds(pl.multiple_of(b * BLK, BLK), BLK)
                for h in range(heads):
                    key_at = pl.ds(h * KEY_CHANNELS, KEY_CHANNELS)
                    decays = shift[s, at, key_at]
                    cumul = jnp.dot(
                        lower.astype(F32), decays, precision=lax.Precision.HIGHEST,
                        preferred_element_type=F32,
                    )
                    total = cumul[BLK - 1 :, :]
                    queries = proj[s, at, key_at].astype(F32) * KEY_CHANNELS ** (-0.5)
                    keys = proj[s, at, pl.ds(key_cols + h * KEY_CHANNELS, KEY_CHANNELS)].astype(F32)
                    values = proj[s, at, pl.ds(2 * key_cols + h * DV, DV)]
                    q_decayed = (queries * jnp.exp(cumul)).astype(BF16)
                    k_decayed = (keys * jnp.exp(-cumul)).astype(BF16)
                    weighted = (keys * jnp.exp(total - cumul)).astype(BF16)
                    scores = lax.dot_general(
                        q_decayed, k_decayed, (((1,), (1,)), ((), ())), preferred_element_type=F32
                    )
                    scores = jnp.where(lower, scores, 0.0).astype(BF16)
                    before = state[h]
                    result = jnp.dot(scores, values, preferred_element_type=F32) + lax.dot_general(
                        q_decayed, before.astype(BF16), (((1,), (1,)), ((), ())), preferred_element_type=F32
                    )
                    state[h] = jnp.exp(total) * before + lax.dot_general(
                        values, weighted, (((0,), (0,)), ((), ())), preferred_element_type=F32
                    )
                    scale = lax.rsqrt(jnp.mean(result * result, axis=-1, keepdims=True) + EPS)
                    gated[s, at, pl.ds(h * DV, DV)] = (
                        result * scale * gain_cols[:, h * DV : (h + 1) * DV]
                    ).astype(BF16)

        def mix_out(s):
            @pl.loop(0, 8)
            def _(b):
                value = jnp.dot(gated[s], wo[b], preferred_element_type=F32).astype(BF16)
                for k in range(4):
                    part[b, k, s] = value[k * rows : (k + 1) * rows]

        def reduce_copies(s):
            return (
                act_copy(("red", s, 0), part.at[:, core, s], near.at[0, s], {"tp": core}),
                act_copy(("red", s, 1), part.at[:, both, s], near.at[1, s], {"tp": core}),
                act_copy(("red", s, 2), part.at[:, chip, s], far.at[s], {"tp": chip}),
            )

        reduce = [reduce_copies(s) for s in range(2)]

        def reduce_far(s):
            reduce[s][1].wait_recv()

            @pl.loop(0, 8)
            def _(b):
                total = part[b, chip, s].astype(F32) + near[1, s, b].astype(F32)
                part[b, chip, s] = total.astype(BF16)

            reduce[s][2].start()

        def reduce_end(s):
            reduce[s][0].wait_recv()
            reduce[s][2].wait_recv()
            for b in range(8):
                cols = pl.ds(b * block, block)
                total = part[b, t, s].astype(F32) + near[0, s, b].astype(F32) + far[s, b].astype(F32)
                hid[s, :, cols] = tok[s, :, cols].astype(F32) + total
                if s == 1:
                    mixed_home[b] = total.astype(BF16)
            if s == 1:
                mixed_copy.start()
            norm_rows(lambda at: hid[s, at, :], ffn_gain, x_ffn, s)
            ffn_gather[s].start()

        project(0)
        rep_end("out")
        rep_own("gate0", "up0")
        shift_copy.wait_recv()
        project(1)
        attend(0)
        rep_own("gate1", "up1")
        complete("out")
        mix_out(0)
        reduce[0][1].start()
        reduce[0][0].start()
        attend(1)
        reduce_far(0)
        mid_end("gate0", "up0")
        mid_own("down")
        mix_out(1)
        reduce[1][1].start()
        reduce[1][0].start()
        reduce_end(0)
        reduce_far(1)
        ffn_gather[0].forward()
        reduce_end(1)
        rep_end("gate0", "up0")
        ffn_gather[0].finish()
        ffn_gather[1].forward()
        complete("gate0", "up0")

        def expand(s, lo, hi):
            @pl.loop(0, seq // 256)
            def _(i):
                at = pl.ds(pl.multiple_of(i * 256, 256), 256)
                x = x_ffn[s, at, :]
                for n in range(lo, hi, 256):
                    cols = pl.ds(n, min(256, hi - n))
                    gate = jnp.dot(x, wg[:, cols], preferred_element_type=F32)
                    up = jnp.dot(x, wu[:, cols], preferred_element_type=F32)
                    act[s, at, cols] = (gate / (1.0 + jnp.exp(-gate)) * up).astype(BF16)

        expand(0, 0, cut)
        mid_end("gate1", "up1")
        rep_own("down")
        ffn_gather[1].finish()
        expand(1, 0, cut)
        mid_end("down")
        rep_end("gate1", "up1")
        complete("gate1", "up1")
        expand(0, cut, hidden_units)
        rep_end("down")
        expand(1, cut, hidden_units)
        for s in range(2):
            for copy in reduce[s]:
                copy.wait_send()

        def piece_copies(i, b):
            return (
                act_copy(("piece", i, 0), part.at[b, core], near2.at[i, 0], {"tp": core}),
                act_copy(("piece", i, 1), part.at[b, both], near2.at[i, 1], {"tp": core}),
                act_copy(("piece", i, 2), part.at[b, chip], far2.at[i], {"tp": chip}),
            )

        pieces = [piece_copies(i, b) for i, (b, _) in enumerate(out_order)]
        waited = ("mid_own", "end_a", "mid_end")
        for i in range(len(out_order) + 2):
            if i < len(out_order):
                b, source = out_order[i]
                if source is not None and source[0] not in waited:
                    incoming("down", *source)
                for s in range(2):
                    value = jnp.dot(act[s], wd[b], preferred_element_type=F32).astype(BF16)
                    for k in range(4):
                        part[b, k, s] = value[k * rows : (k + 1) * rows]
                pieces[i][1].start()
                pieces[i][0].start()
            if 1 <= i <= len(out_order):
                b = out_order[i - 1][0]
                pieces[i - 1][1].wait_recv()
                part[b, chip] = (part[b, chip].astype(F32) + near2[i - 1, 1].astype(F32)).astype(BF16)
                pieces[i - 1][2].start()
            if i >= 2:
                b = out_order[i - 2][0]
                pieces[i - 2][0].wait_recv()
                pieces[i - 2][2].wait_recv()
                total = part[b, t].astype(F32) + near2[i - 2, 0].astype(F32) + far2[i - 2].astype(F32)
                cols = pl.ds(pl.multiple_of(b * block, block), block)
                ffn_home[b] = total[1].astype(BF16)
                home_copies[i - 2].start()
                out[:, cols] = hid[0, :, cols] + total[0]
        for gather in mix_gather + ffn_gather:
            gather.drain()
        for copies in pieces:
            for copy in copies:
                copy.wait_send()
        mixed_copy.wait_send()
        for copy in home_copies:
            copy.wait_send()
        for copy in sent:
            copy.wait_send()


def per_device_kernel(
    tokens, mix_gain, w_query, w_key, w_value, w_decay_down, w_decay_up, decay_bias,
    decay_shift, head_gain, w_mix_out, ffn_gain, w_gate, w_up, w_down,
):
    rows, width = tokens.shape
    planes, tps = lax.axis_size("fs"), lax.axis_size("tp")
    key_cols, value_cols, hidden_units = w_query.shape[1], w_value.shape[1], w_gate.shape[1]
    depth = w_query.shape[0]
    seq = rows * tps
    blocks = 2 * planes
    block = width // blocks
    any_spec = pl.BlockSpec(memory_space=pl.ANY)
    vmem_spec = pl.BlockSpec(memory_space=pltpu.VMEM)
    large = {0, 2, 3, 4, 8, 10, 12, 13, 14}
    args = (
        tokens, mix_gain.reshape(1, -1), w_query, w_key, w_value, w_decay_down, w_decay_up,
        decay_bias.reshape(1, -1), decay_shift, head_gain.reshape(1, -1), w_mix_out,
        ffn_gain.reshape(1, -1), w_gate, w_up, w_down,
    )
    return pl.pallas_call(
        layer_kernel,
        out_shape=jax.ShapeDtypeStruct((rows, width), F32),
        in_specs=[any_spec if i in large else vmem_spec for i in range(len(args))],
        out_specs=vmem_spec,
        scratch_shapes=[
            pltpu.VMEM((planes * depth, 2 * key_cols + value_cols), BF16),
            pltpu.VMEM((blocks, value_cols, block), BF16),
            pltpu.VMEM((planes * depth, hidden_units), BF16),
            pltpu.VMEM((planes * depth, hidden_units), BF16),
            pltpu.VMEM((blocks, hidden_units, block), BF16),
            pltpu.VMEM((2, rows, width), BF16),
            pltpu.VMEM((2, seq, key_cols), F32),
            pltpu.VMEM((2, seq, width), BF16),
            pltpu.VMEM((2, seq, width), BF16),
            pltpu.VMEM((2, seq, 2 * key_cols + value_cols), BF16),
            pltpu.VMEM((2, seq, value_cols), BF16),
            pltpu.VMEM((blocks, tps, 2, rows, block), BF16),
            pltpu.VMEM((2, 2, blocks, rows, block), BF16),
            pltpu.VMEM((2, blocks, rows, block), BF16),
            pltpu.VMEM((blocks, 2, 2, rows, block), BF16),
            pltpu.VMEM((blocks, 2, rows, block), BF16),
            pltpu.VMEM((2, seq, hidden_units), BF16),
            pltpu.VMEM((2, rows, width), F32),
            pltpu.VMEM((blocks, rows, block), BF16),
            pltpu.VMEM((blocks, rows, block), BF16),
            pltpu.VMEM((key_cols // KEY_CHANNELS, DV, KEY_CHANNELS), F32),
            pltpu.SemaphoreType.DMA((16,)),
            pltpu.SemaphoreType.DMA((len(PARTS) * len(KINDS),)),
            pltpu.SemaphoreType.DMA((len(PARTS) * len(KINDS),)),
            pltpu.SemaphoreType.DMA((64,)),
            pltpu.SemaphoreType.DMA((64,)),
        ],
        compiler_params=pltpu.CompilerParams(
            collective_id=0, has_side_effects=True, vmem_limit_bytes=67043328
        ),
    )(*args)


def solution(mesh):
    shape = dict(mesh.shape)
    small = shape["rep"] == 2 and shape["fs"] == 4 and shape["tp"] == 4
    return jax.shard_map(
        per_device_kernel if small else per_device,
        mesh=mesh,
        in_specs=(
            P(("rep", "fs", "tp"), None),
            P(),
            P("fs", "tp"),
            P("fs", "tp"),
            P("fs", "tp"),
            P(),
            P(),
            P(),
            P(("rep", "fs"), "tp"),
            P(),
            P("tp", "fs"),
            P(),
            P("fs", "tp"),
            P("fs", "tp"),
            P("tp", "fs"),
        ),
        out_specs=P(("rep", "fs", "tp"), None),
        check_vma=False,
    )
```

```python
import jax
import jax.numpy as jnp
from jax import lax
from jax.experimental import pallas as pl
from jax.experimental.pallas import tpu as pltpu
from jax.sharding import PartitionSpec as P

KEY_CHANNELS = 128
DV = 256
BLK = 64


EPS = 1e-06
TAU = 16.0


def rms_norm(values, gain):
    return values * lax.rsqrt(jnp.mean(values * values, axis=-1, keepdims=True) + EPS) * gain


def recurrence(query_proj, key_proj, value_proj, log_decay, head_count):
    seq_rows = query_proj.shape[0]
    blocks = seq_rows // BLK
    exact = lax.Precision.HIGHEST
    queries = query_proj.astype(jnp.float32).reshape(
        blocks, BLK, head_count, KEY_CHANNELS
    ) * KEY_CHANNELS ** (-0.5)
    keys = key_proj.astype(jnp.float32).reshape(blocks, BLK, head_count, KEY_CHANNELS)
    values = value_proj.astype(jnp.float32).reshape(blocks, BLK, head_count, DV)
    decays = log_decay.reshape(blocks, BLK, head_count, KEY_CHANNELS)
    lower = (jnp.arange(BLK)[:, None] >= jnp.arange(BLK)[None, :]).astype(jnp.float32)
    cumul = jnp.einsum("cs,bshd->bchd", lower, decays, precision=exact)
    totals = cumul[:, -1]
    weighted = keys * jnp.exp(totals[:, None] - cumul)
    updates = jnp.einsum("bchd,bche->bhde", weighted, values, precision=exact)
    state = jnp.zeros_like(updates[0])
    previous = []
    for block in range(blocks):
        previous.append(state)
        state = jnp.exp(totals[block])[..., None] * state + updates[block]
    previous = jnp.stack(previous)
    q_decayed = queries * jnp.exp(cumul)
    k_decayed = keys * jnp.exp(-cumul)
    scores = jnp.einsum("bchd,bshd->bhcs", q_decayed, k_decayed, precision=exact)
    scores = scores * lower
    inner = jnp.einsum("bhcs,bshe->bche", scores, values, precision=exact)
    carried = jnp.einsum("bchd,bhde->bche", q_decayed, previous, precision=exact)
    return (inner + carried).reshape(seq_rows, head_count, DV)


def shift(values, axis, distance):
    count = lax.axis_size(axis)
    return lax.ppermute(values, axis, [(i, (i + distance) % count) for i in range(count)])


def swap_core(values):
    return lax.ppermute(values, "tp", [(i, i ^ 1) for i in range(lax.axis_size("tp"))])


def gather_rows(block):
    count = lax.axis_size("tp")
    index = lax.axis_index("tp")
    chips, core, chip = count // 2, index % 2, index // 2
    rows = block.shape[0]
    mine = [block] + [shift(block, "tp", 2 * k) for k in range(1, chips)]
    whole = jnp.zeros((count * rows,) + block.shape[1:], block.dtype)
    for k, piece in enumerate(mine):
        source = (chip - k) % chips
        theirs = swap_core(piece)
        whole = lax.dynamic_update_slice_in_dim(whole, piece, (2 * source + core) * rows, 0)
        whole = lax.dynamic_update_slice_in_dim(whole, theirs, (2 * source + 1 - core) * rows, 0)
    return whole


def scatter_sum(partial):
    count = lax.axis_size("tp")
    index = lax.axis_index("tp")
    chips, core, chip = count // 2, index % 2, index // 2
    rows = partial.shape[0] // count
    blocks = partial.astype(jnp.bfloat16).reshape(chips, 2, rows, partial.shape[1])
    away = lax.dynamic_index_in_dim(blocks, 1 - core, 1, keepdims=False)
    kept = lax.dynamic_index_in_dim(blocks, core, 1, keepdims=False).astype(jnp.float32)
    pair = kept + swap_core(away).astype(jnp.float32)
    rounded = pair.astype(jnp.bfloat16)
    total = lax.dynamic_index_in_dim(pair, chip, 0, keepdims=False)
    for k in range(1, chips):
        outgoing = lax.dynamic_index_in_dim(rounded, (chip + k) % chips, 0, keepdims=False)
        total = total + shift(outgoing, "tp", 2 * k).astype(jnp.float32)
    return total


def row_parts(weight):
    reps = lax.axis_size("rep")
    share = weight.shape[0] // reps
    own = lax.dynamic_slice_in_dim(weight, lax.axis_index("rep") * share, share, 0)
    own = lax.all_gather(own, "fs", axis=0, tiled=True)
    return [own] + [shift(own, "rep", k) for k in range(1, reps)]


def column_parts(weight):
    reps = lax.axis_size("rep")
    share = weight.shape[1] // reps
    own = lax.dynamic_slice_in_dim(weight, lax.axis_index("rep") * share, share, 1)
    own = lax.all_gather(own, "fs", axis=0, tiled=False)
    return [own] + [shift(own, "rep", k) for k in range(1, reps)]


def input_parts(values):
    reps, groups = lax.axis_size("rep"), lax.axis_size("fs")
    share = values.shape[1] // (reps * groups)
    layouts = [
        jnp.concatenate(
            [
                values[:, (g * reps + j) * share : (g * reps + j + 1) * share]
                for g in range(groups)
            ],
            axis=1,
        )
        for j in range(reps)
    ]
    index = lax.axis_index("rep")
    return [
        lax.select_n(jnp.full((), (index - k) % reps, jnp.int32), *layouts) if reps > 2
        else (jnp.where((index - k) % reps == 0, layouts[0], layouts[-1]))
        for k in range(reps)
    ]


def dots(inputs, weights):
    total = jnp.dot(inputs[0], weights[0], preferred_element_type=jnp.float32)
    for left, right in zip(inputs[1:], weights[1:]):
        total = total + jnp.dot(left, right, preferred_element_type=jnp.float32)
    return total


def project_out(values, weights):
    reps = lax.axis_size("rep")
    index = lax.axis_index("rep")
    sums = []
    for weight in weights:
        partial = jnp.concatenate(
            [
                jnp.dot(values, weight[g], preferred_element_type=jnp.float32)
                for g in range(weight.shape[0])
            ],
            axis=1,
        )
        sums.append(scatter_sum(partial))
    share = weights[0].shape[2]
    ordered = []
    for j in range(reps):
        if reps == 2:
            ordered.append(jnp.where(index == j, sums[0], sums[1]))
        else:
            ordered.append(lax.select_n((index - j) % reps, *sums))
    pieces = []
    for g in range(weights[0].shape[0]):
        for j in range(reps):
            pieces.append(ordered[j][:, g * share : (g + 1) * share])
    return jnp.concatenate(pieces, axis=1)


def per_device(
    tokens,
    mix_gain,
    w_query,
    w_key,
    w_value,
    w_decay_down,
    w_decay_up,
    decay_bias,
    decay_shift,
    head_gain,
    w_mix_out,
    ffn_gain,
    w_gate,
    w_up,
    w_down,
):
    tp_index = lax.axis_index("tp")
    key_cols = w_query.shape[1]
    value_cols = w_value.shape[1]
    heads_dev = key_cols // KEY_CHANNELS
    own_tokens = tokens.astype(jnp.float32)
    qkv_weights = row_parts(jnp.concatenate([w_query, w_key, w_value], axis=1))
    out_weights = column_parts(w_mix_out)
    gate_weights = row_parts(w_gate)
    up_weights = row_parts(w_up)
    down_weights = column_parts(w_down)
    normed = gather_rows(rms_norm(own_tokens, mix_gain).astype(jnp.bfloat16))
    seq_rows = normed.shape[0]
    low_rank = jnp.dot(normed, w_decay_down, preferred_element_type=jnp.float32).astype(
        jnp.bfloat16
    )
    up_columns = lax.dynamic_slice_in_dim(w_decay_up, tp_index * key_cols, key_cols, 1)
    bias_columns = lax.dynamic_slice_in_dim(decay_bias, tp_index * key_cols, key_cols, 0)
    pre_decay = jnp.dot(low_rank, up_columns, preferred_element_type=jnp.float32) + bias_columns
    log_decay = jax.nn.log_sigmoid(pre_decay) / TAU + decay_shift
    projected = dots(input_parts(normed), qkv_weights).astype(jnp.bfloat16)
    query_proj = projected[:, :key_cols]
    key_proj = projected[:, key_cols : 2 * key_cols]
    value_proj = projected[:, 2 * key_cols :]
    head_out = recurrence(query_proj, key_proj, value_proj, log_decay, heads_dev)
    gain_columns = lax.dynamic_slice_in_dim(head_gain, tp_index * value_cols, value_cols, 0)
    gated = rms_norm(head_out, gain_columns.reshape(heads_dev, DV)).astype(jnp.bfloat16)
    gated = gated.reshape(seq_rows, value_cols)
    hidden = own_tokens + project_out(gated, out_weights)
    normed_ffn = gather_rows(rms_norm(hidden, ffn_gain).astype(jnp.bfloat16))
    ffn_inputs = input_parts(normed_ffn)
    gate_proj = dots(ffn_inputs, gate_weights)
    up_proj = dots(ffn_inputs, up_weights)
    activated = (jax.nn.silu(gate_proj) * up_proj).astype(jnp.bfloat16)
    return hidden + project_out(activated, down_weights)


BF16 = jnp.bfloat16
F32 = jnp.float32
MESH_ID = pl.DeviceIdType.MESH
KINDS = ("end_a", "end_b", "mid_own", "mid_end", "rep_own", "rep_end")
PARTS = ("qkv0", "qkv1", "out", "gate0", "up0", "gate1", "up1", "down0", "down1")
VIA_REP = ("out",)


def layer_kernel(
    tokens, mix_gain, w_query, w_key, w_value, w_decay_down, w_decay_up, decay_bias,
    decay_shift, head_gain, w_mix_out, ffn_gain, w_gate, w_up, w_down,
    out,
    wq, wo, wg, wu, wd, tok, shift, x_mix, x_ffn, proj, gated, part, near, far, near2, far2,
    act, hid, mixed_home, ffn_home, state,
    load_sem, w_send, w_recv, a_send, a_recv,
):
    r, z, t = lax.axis_index("rep"), lax.axis_index("fs"), lax.axis_index("tp")
    depth, key_cols = w_query.shape
    value_cols = w_value.shape[1]
    rows, width = tokens.shape
    seq = rows * 4
    hidden_units = w_gate.shape[1]
    block = width // 8
    half_rows = depth // 2
    cut = (hidden_units // 256 + 1) // 2 * 256
    heads = key_cols // KEY_CHANNELS
    zc = 1 + z // 2
    ze = 3 * (z // 2)
    zo, zf = 3 - zc, 3 - ze
    other_r = 1 - r
    core = t + 1 - 2 * lax.rem(t, 2)
    chip = lax.rem(t + 2, 4)
    both = 3 - t
    pair_z = z + 1 - 2 * lax.rem(z, 2)
    is_centre = jnp.logical_and(z >= 1, z <= 2)

    barrier = pltpu.get_barrier_semaphore()
    for partner in ({"fs": pair_z}, {"fs": 3 - z}, {"rep": other_r}, {"tp": core}, {"tp": chip}):
        pl.semaphore_signal(barrier, inc=1, device_id=partner, device_id_type=MESH_ID)

    def region(name, plane, half):
        at = pl.multiple_of(plane * depth + half * half_rows, half_rows)
        if name.startswith("qkv"):
            piece = half_rows // 2
            return wq.at[pl.ds(pl.multiple_of(at + int(name[-1]) * piece, piece), piece), :]
        if name == "out":
            return wo.at[2 * plane + half]
        if name.startswith("down"):
            piece = hidden_units // 2
            return wd.at[2 * plane + half, pl.ds(int(name[-1]) * piece, piece)]
        ref = wg if name.startswith("gate") else wu
        if name.endswith("0"):
            return ref.at[pl.ds(at, half_rows), pl.ds(0, cut)]
        return ref.at[pl.ds(at, half_rows), pl.ds(cut, hidden_units - cut)]

    def weight_copy(name, kind, plane, half, device):
        ref = region(name, plane, half)
        index = PARTS.index(name) * len(KINDS) + KINDS.index(kind)
        return pltpu.make_async_remote_copy(
            src_ref=ref, dst_ref=ref, send_sem=w_send.at[index], recv_sem=w_recv.at[index],
            device_id=device, device_id_type=MESH_ID,
        )

    act_ids = {}

    def act_copy(key, src, dst, device):
        index = act_ids.setdefault(key, len(act_ids))
        return pltpu.make_async_remote_copy(
            src_ref=src, dst_ref=dst, send_sem=a_send.at[index], recv_sem=a_recv.at[index],
            device_id=device, device_id_type=MESH_ID,
        )

    at_z = pl.multiple_of(z * depth, depth)
    loads = {}

    def load(name, src, dst):
        copy = pltpu.make_async_copy(src, dst, load_sem.at[len(loads)])
        copy.start()
        loads[name] = copy

    load("q", w_query, wq.at[pl.ds(at_z, depth), pl.ds(0, key_cols)])
    load("k", w_key, wq.at[pl.ds(at_z, depth), pl.ds(key_cols, key_cols)])
    load("v", w_value, wq.at[pl.ds(at_z, depth), pl.ds(2 * key_cols, value_cols)])
    load("tok", tokens, tok.at[0])
    load("o0", w_mix_out.at[:, pl.ds(0, block)], wo.at[2 * z])
    load("o1", w_mix_out.at[:, pl.ds(block, block)], wo.at[2 * z + 1])
    load("shift", decay_shift, shift.at[0])
    load("g", w_gate, wg.at[pl.ds(at_z, depth), :])
    load("u", w_up, wu.at[pl.ds(at_z, depth), :])
    load("d0", w_down.at[:, pl.ds(0, block)], wd.at[2 * z])
    load("d1", w_down.at[:, pl.ds(block, block)], wd.at[2 * z + 1])
    pl.semaphore_wait(barrier, 5)
    for name in ("q", "k", "v"):
        loads[name].wait()

    tok_copy = act_copy("tok", tok.at[0], tok.at[1], {"fs": pair_z})
    shift_copy = act_copy("shift", shift.at[0], shift.at[1], {"fs": pair_z})

    out_order = [
        (2 * zc, None), (2 * zc + 1, None),
        (2 * zo + r, None), (2 * ze + r, None), (2 * zo + other_r, ("rep_own", zo, other_r)),
        (2 * zf + r, None), (2 * ze + other_r, ("end_b", ze, other_r)),
        (2 * zf + other_r, ("rep_end", zf, other_r)),
    ]
    mixed_copy = act_copy("mixed", mixed_home, mixed_home, {"fs": pair_z})
    home_copies = [
        act_copy(("home", i), ffn_home.at[b], ffn_home.at[b], {"fs": pair_z})
        for i, (b, _) in enumerate(out_order)
    ]

    @pl.when(jnp.logical_not(is_centre))
    def _():
        sent = []

        def send(name, kind, half):
            copy = weight_copy(name, kind, z, half, {"fs": pair_z})
            copy.start()
            sent.append(copy)

        send("qkv0", "end_a", r)
        send("qkv1", "end_a", r)
        loads["o0"].wait()
        loads["o1"].wait()
        send("out", "end_a", r)
        loads["tok"].wait()
        tok_copy.start()
        send("qkv0", "end_b", other_r)
        send("qkv1", "end_b", other_r)
        loads["shift"].wait()
        shift_copy.start()
        loads["g"].wait()
        loads["u"].wait()
        send("gate0", "end_a", r)
        send("up0", "end_a", r)
        send("gate1", "end_a", r)
        send("up1", "end_a", r)
        send("gate0", "end_b", other_r)
        send("up0", "end_b", other_r)
        send("gate1", "end_b", other_r)
        send("up1", "end_b", other_r)
        loads["d0"].wait()
        loads["d1"].wait()
        send("down0", "end_a", r)
        send("down1", "end_a", r)
        send("down0", "end_b", other_r)
        send("down1", "end_b", other_r)
        mixed_copy.wait_recv()
        for i, (b, _) in enumerate(out_order):
            home_copies[i].wait_recv()
            cols = pl.ds(pl.multiple_of(b * block, block), block)
            out[:, cols] = (
                tok[0, :, cols].astype(F32) + mixed_home[b].astype(F32) + ffn_home[b].astype(F32)
            )
        tok_copy.wait_send()
        shift_copy.wait_send()
        for copy in sent:
            copy.wait_send()

    @pl.when(is_centre)
    def _():
        sent = []

        def incoming(name, kind, plane, half):
            weight_copy(name, kind, plane, half, {"fs": pair_z}).wait_recv()

        def send(name, kind, plane, half, device):
            copy = weight_copy(name, kind, plane, half, device)
            copy.start()
            sent.append(copy)

        def mid_own(*parts):
            for name in parts:
                send(name, "mid_own", z, r, {"fs": zo})

        def mid_end(*parts):
            for name in parts:
                incoming(name, "end_a", ze, r)
                send(name, "mid_end", ze, r, {"fs": zo})

        def rep_own(*parts):
            for name in parts:
                incoming(name, "mid_own", zo, r)
                send(name, "rep_own", zo, r, {"rep": other_r})

        def rep_end(*parts):
            for name in parts:
                incoming(name, "mid_end", zf, r)
                send(name, "rep_end", zf, r, {"rep": other_r})

        def rep_end_b(*parts):
            for name in parts:
                send(name, "end_b", ze, r, {"rep": other_r})

        def complete(*parts):
            for name in parts:
                incoming(name, "end_b", ze, other_r)
                incoming(name, "rep_own", zo, other_r)
                incoming(name, "rep_end", zf, other_r)

        def norm_rows(load_rows, gain, dst, s):
            @pl.loop(0, rows // 16)
            def _(i):
                values = load_rows(pl.ds(pl.multiple_of(i * 16, 16), 16))
                scale = lax.rsqrt(jnp.mean(values * values, axis=-1, keepdims=True) + EPS)
                at = pl.multiple_of(t * rows + i * 16, 16)
                dst[s, pl.ds(at, 16), :] = (values * scale * gain[...]).astype(BF16)

        class Gather:
            def __init__(self, key, ref, s):
                def rows_of(device):
                    return ref.at[s, pl.ds(pl.multiple_of(device * rows, rows), rows), :]

                mine, theirs = rows_of(t), rows_of(chip)
                self.to_chip = act_copy((key, s, "chip"), mine, mine, {"tp": chip})
                self.to_core = act_copy((key, s, "core"), mine, mine, {"tp": core})
                self.pass_on = act_copy((key, s, "pass"), theirs, theirs, {"tp": core})
                self.from_chip = act_copy((key, s, "chip"), theirs, theirs, {"tp": chip})
                self.from_core = act_copy((key, s, "core"), rows_of(core), rows_of(core), {"tp": core})
                self.passed = act_copy((key, s, "pass"), rows_of(both), rows_of(both), {"tp": core})

            def start(self):
                self.to_chip.start()
                self.to_core.start()

            def forward(self):
                self.from_chip.wait_recv()
                self.pass_on.start()

            def finish(self):
                self.from_core.wait_recv()
                self.passed.wait_recv()

            def drain(self):
                self.to_chip.wait_send()
                self.to_core.wait_send()
                self.pass_on.wait_send()

        mid_own("qkv0", "qkv1")
        loads["tok"].wait()
        norm_rows(lambda at: tok[0, at, :].astype(F32), mix_gain, x_mix, 0)
        mix_gather = [Gather("mix", x_mix, s) for s in range(2)]
        ffn_gather = [Gather("ffn", x_ffn, s) for s in range(2)]
        mix_gather[0].start()
        for name in ("o0", "o1", "shift", "g", "u", "d0", "d1"):
            loads[name].wait()
        bias = decay_bias[:, pl.ds(pl.multiple_of(t * key_cols, key_cols), key_cols)]
        up_cols = w_decay_up[:, pl.ds(pl.multiple_of(t * key_cols, key_cols), key_cols)]

        def project(s):
            @pl.loop(0, seq // 256)
            def _(i):
                at = pl.ds(pl.multiple_of(i * 256, 256), 256)
                x = x_mix[s, at, :]
                for n in range(0, 2 * key_cols + value_cols, 512):
                    cols = pl.ds(n, 512)
                    proj[s, at, cols] = jnp.dot(x, wq[:, cols], preferred_element_type=F32).astype(BF16)
                low = lax.dot_general(
                    x, w_decay_down[...], (((1,), (1,)), ((), ())), preferred_element_type=F32
                ).astype(BF16)
                pre = jnp.dot(low, up_cols, preferred_element_type=F32) + bias
                log_sig = jnp.minimum(pre, 0.0) - jnp.log1p(jnp.exp(-jnp.abs(pre)))
                shift[s, at, :] = log_sig / TAU + shift[s, at, :]

        lower = (
            lax.broadcasted_iota(jnp.int32, (BLK, BLK), 0) >= lax.broadcasted_iota(jnp.int32, (BLK, BLK), 1)
        )
        gain_cols = head_gain[:, pl.ds(pl.multiple_of(t * value_cols, value_cols), value_cols)]

        def attend(s):
            state[...] = jnp.zeros_like(state)

            @pl.loop(0, seq // BLK)
            def _(b):
                at = pl.ds(pl.multiple_of(b * BLK, BLK), BLK)
                for h in range(heads):
                    key_at = pl.ds(h * KEY_CHANNELS, KEY_CHANNELS)
                    decays = shift[s, at, key_at]
                    cumul = jnp.dot(
                        lower.astype(F32), decays, precision=lax.Precision.HIGHEST,
                        preferred_element_type=F32,
                    )
                    total = cumul[BLK - 1 :, :]
                    queries = proj[s, at, key_at].astype(F32) * KEY_CHANNELS ** (-0.5)
                    keys = proj[s, at, pl.ds(key_cols + h * KEY_CHANNELS, KEY_CHANNELS)].astype(F32)
                    values = proj[s, at, pl.ds(2 * key_cols + h * DV, DV)]
                    q_decayed = (queries * jnp.exp(cumul)).astype(BF16)
                    k_decayed = (keys * jnp.exp(-cumul)).astype(BF16)
                    weighted = (keys * jnp.exp(total - cumul)).astype(BF16)
                    scores = lax.dot_general(
                        q_decayed, k_decayed, (((1,), (1,)), ((), ())), preferred_element_type=F32
                    )
                    scores = jnp.where(lower, scores, 0.0).astype(BF16)
                    before = state[h]
                    result = jnp.dot(scores, values, preferred_element_type=F32) + lax.dot_general(
                        q_decayed, before.astype(BF16), (((1,), (1,)), ((), ())), preferred_element_type=F32
                    )
                    state[h] = jnp.exp(total) * before + lax.dot_general(
                        values, weighted, (((0,), (0,)), ((), ())), preferred_element_type=F32
                    )
                    scale = lax.rsqrt(jnp.mean(result * result, axis=-1, keepdims=True) + EPS)
                    gated[s, at, pl.ds(h * DV, DV)] = (
                        result * scale * gain_cols[:, h * DV : (h + 1) * DV]
                    ).astype(BF16)

        def mix_out(s):
            @pl.loop(0, 8)
            def _(b):
                value = jnp.dot(gated[s], wo[b], preferred_element_type=F32).astype(BF16)
                for k in range(4):
                    part[b, k, s] = value[k * rows : (k + 1) * rows]

        def reduce_copies(s):
            return (
                act_copy(("red", s, 0), part.at[:, core, s], near.at[0, s], {"tp": core}),
                act_copy(("red", s, 1), part.at[:, both, s], near.at[1, s], {"tp": core}),
                act_copy(("red", s, 2), part.at[:, chip, s], far.at[s], {"tp": chip}),
            )

        reduce = [reduce_copies(s) for s in range(2)]

        def reduce_far(s):
            reduce[s][1].wait_recv()

            @pl.loop(0, 8)
            def _(b):
                total = part[b, chip, s].astype(F32) + near[1, s, b].astype(F32)
                part[b, chip, s] = total.astype(BF16)

            reduce[s][2].start()

        def reduce_end(s):
            reduce[s][0].wait_recv()
            reduce[s][2].wait_recv()
            for b in range(8):
                cols = pl.ds(b * block, block)
                total = part[b, t, s].astype(F32) + near[0, s, b].astype(F32) + far[s, b].astype(F32)
                hid[s, :, cols] = tok[s, :, cols].astype(F32) + total
                if s == 1:
                    mixed_home[b] = total.astype(BF16)
            if s == 1:
                mixed_copy.start()
            norm_rows(lambda at: hid[s, at, :], ffn_gain, x_ffn, s)
            ffn_gather[s].start()

        def expand(s, lo, hi):
            @pl.loop(0, seq // 256)
            def _(i):
                at = pl.ds(pl.multiple_of(i * 256, 256), 256)
                x = x_ffn[s, at, :]
                for n in range(lo, hi, 256):
                    cols = pl.ds(n, min(256, hi - n))
                    gate = jnp.dot(x, wg[:, cols], preferred_element_type=F32)
                    up = jnp.dot(x, wu[:, cols], preferred_element_type=F32)
                    act[s, at, cols] = (gate / (1.0 + jnp.exp(-gate)) * up).astype(BF16)

        def piece_copies(i, b):
            return (
                act_copy(("piece", i, 0), part.at[b, core], near2.at[i, 0], {"tp": core}),
                act_copy(("piece", i, 1), part.at[b, both], near2.at[i, 1], {"tp": core}),
                act_copy(("piece", i, 2), part.at[b, chip], far2.at[i], {"tp": chip}),
            )

        pieces = [piece_copies(i, b) for i, (b, _) in enumerate(out_order)]

        def reduce_start(s):
            reduce[s][1].start()
            reduce[s][0].start()

        def reduce_drain():
            for s in range(2):
                for copy in reduce[s]:
                    copy.wait_send()

        def piece_dot(i):
            b, source = out_order[i]
            if source is not None:
                incoming("down0", *source)
                incoming("down1", *source)
            for s in range(2):
                value = jnp.dot(act[s], wd[b], preferred_element_type=F32).astype(BF16)
                for k in range(4):
                    part[b, k, s] = value[k * rows : (k + 1) * rows]
            pieces[i][1].start()
            pieces[i][0].start()

        def piece_far(i):
            b = out_order[i][0]
            pieces[i][1].wait_recv()
            part[b, chip] = (part[b, chip].astype(F32) + near2[i, 1].astype(F32)).astype(BF16)
            pieces[i][2].start()

        def piece_end(i):
            b = out_order[i][0]
            pieces[i][0].wait_recv()
            pieces[i][2].wait_recv()
            total = part[b, t].astype(F32) + near2[i, 0].astype(F32) + far2[i].astype(F32)
            cols = pl.ds(pl.multiple_of(b * block, block), block)
            ffn_home[b] = total[1].astype(BF16)
            home_copies[i].start()
            out[:, cols] = hid[0, :, cols] + total[0]

        mid_end("qkv0")
        rep_own("qkv0")
        mid_end("qkv1")
        rep_own("qkv1")
        mix_gather[0].forward()
        mid_own("out")
        mid_end("out")
        mid_own("gate0", "up0")
        rep_end("qkv0")
        rep_end("qkv1")
        tok_copy.wait_recv()
        norm_rows(lambda at: tok[1, at, :].astype(F32), mix_gain, x_mix, 1)
        mix_gather[1].start()
        rep_own("out")
        rep_end_b("out")
        rep_end("out")
        mid_own("gate1", "up1")
        mix_gather[0].finish()
        complete("qkv0", "qkv1")
        project(0)
        mix_gather[1].forward()
        rep_own("gate0")
        attend(0)
        complete("out")
        mix_out(0)
        reduce_start(0)
        mix_gather[1].finish()
        shift_copy.wait_recv()
        project(1)
        reduce_far(0)
        rep_own("up0")
        attend(1)
        mix_out(1)
        reduce_start(1)
        rep_own("gate1")
        mid_end("gate0")
        reduce_far(1)
        rep_own("up1")
        reduce_end(0)
        mid_end("up0")
        rep_end("gate0")
        reduce_end(1)
        mid_end("gate1", "up1")
        mid_own("down0", "down1")
        rep_end("up0")
        ffn_gather[0].forward()
        rep_end("gate1")
        ffn_gather[0].finish()
        ffn_gather[1].forward()
        rep_end("up1")
        complete("gate0", "up0")
        expand(0, 0, cut)
        ffn_gather[1].finish()
        expand(1, 0, cut)
        rep_own("down0")
        rep_own("down1")
        complete("gate1", "up1")
        expand(0, cut, hidden_units)
        expand(1, cut, hidden_units)
        reduce_drain()
        mid_end("down0")
        piece_dot(0)
        piece_dot(1)
        piece_far(0)
        piece_dot(2)
        piece_far(1)
        piece_end(0)
        piece_far(2)
        piece_end(1)
        mid_end("down1")
        rep_end("down0")
        piece_dot(3)
        piece_dot(4)
        piece_far(3)
        piece_end(2)
        rep_end("down1")
        piece_dot(5)
        piece_far(4)
        piece_end(3)
        piece_dot(6)
        piece_far(5)
        piece_end(4)
        piece_dot(7)
        piece_far(6)
        piece_end(5)
        piece_far(7)
        piece_end(6)
        piece_end(7)
        for gather in mix_gather + ffn_gather:
            gather.drain()
        for copies in pieces:
            for copy in copies:
                copy.wait_send()
        mixed_copy.wait_send()
        for copy in home_copies:
            copy.wait_send()
        for copy in sent:
            copy.wait_send()


def per_device_kernel(
    tokens, mix_gain, w_query, w_key, w_value, w_decay_down, w_decay_up, decay_bias,
    decay_shift, head_gain, w_mix_out, ffn_gain, w_gate, w_up, w_down,
):
    rows, width = tokens.shape
    planes, tps = lax.axis_size("fs"), lax.axis_size("tp")
    key_cols, value_cols, hidden_units = w_query.shape[1], w_value.shape[1], w_gate.shape[1]
    depth = w_query.shape[0]
    seq = rows * tps
    blocks = 2 * planes
    block = width // blocks
    any_spec = pl.BlockSpec(memory_space=pl.ANY)
    vmem_spec = pl.BlockSpec(memory_space=pltpu.VMEM)
    large = {0, 2, 3, 4, 8, 10, 12, 13, 14}
    args = (
        tokens, mix_gain.reshape(1, -1), w_query, w_key, w_value, w_decay_down.T, w_decay_up,
        decay_bias.reshape(1, -1), decay_shift, head_gain.reshape(1, -1), w_mix_out,
        ffn_gain.reshape(1, -1), w_gate, w_up, w_down,
    )
    return pl.pallas_call(
        layer_kernel,
        out_shape=jax.ShapeDtypeStruct((rows, width), F32),
        in_specs=[any_spec if i in large else vmem_spec for i in range(len(args))],
        out_specs=vmem_spec,
        scratch_shapes=[
            pltpu.VMEM((planes * depth, 2 * key_cols + value_cols), BF16),
            pltpu.VMEM((blocks, value_cols, block), BF16),
            pltpu.VMEM((planes * depth, hidden_units), BF16),
            pltpu.VMEM((planes * depth, hidden_units), BF16),
            pltpu.VMEM((blocks, hidden_units, block), BF16),
            pltpu.VMEM((2, rows, width), BF16),
            pltpu.VMEM((2, seq, key_cols), F32),
            pltpu.VMEM((2, seq, width), BF16),
            pltpu.VMEM((2, seq, width), BF16),
            pltpu.VMEM((2, seq, 2 * key_cols + value_cols), BF16),
            pltpu.VMEM((2, seq, value_cols), BF16),
            pltpu.VMEM((blocks, tps, 2, rows, block), BF16),
            pltpu.VMEM((2, 2, blocks, rows, block), BF16),
            pltpu.VMEM((2, blocks, rows, block), BF16),
            pltpu.VMEM((blocks, 2, 2, rows, block), BF16),
            pltpu.VMEM((blocks, 2, rows, block), BF16),
            pltpu.VMEM((2, seq, hidden_units), BF16),
            pltpu.VMEM((2, rows, width), F32),
            pltpu.VMEM((blocks, rows, block), BF16),
            pltpu.VMEM((blocks, rows, block), BF16),
            pltpu.VMEM((key_cols // KEY_CHANNELS, DV, KEY_CHANNELS), F32),
            pltpu.SemaphoreType.DMA((16,)),
            pltpu.SemaphoreType.DMA((len(PARTS) * len(KINDS),)),
            pltpu.SemaphoreType.DMA((len(PARTS) * len(KINDS),)),
            pltpu.SemaphoreType.DMA((64,)),
            pltpu.SemaphoreType.DMA((64,)),
        ],
        compiler_params=pltpu.CompilerParams(
            collective_id=0, has_side_effects=True, vmem_limit_bytes=67043328
        ),
    )(*args)


def solution(mesh):
    shape = dict(mesh.shape)
    small = shape["rep"] == 2 and shape["fs"] == 4 and shape["tp"] == 4
    return jax.shard_map(
        per_device_kernel if small else per_device,
        mesh=mesh,
        in_specs=(
            P(("rep", "fs", "tp"), None),
            P(),
            P("fs", "tp"),
            P("fs", "tp"),
            P("fs", "tp"),
            P(),
            P(),
            P(),
            P(("rep", "fs"), "tp"),
            P(),
            P("tp", "fs"),
            P(),
            P("fs", "tp"),
            P("fs", "tp"),
            P("tp", "fs"),
        ),
        out_specs=P(("rep", "fs", "tp"), None),
        check_vma=False,
    )
```

```python
import jax
import jax.numpy as jnp
from jax import lax
from jax.experimental import pallas as pl
from jax.experimental.pallas import tpu as pltpu
from jax.sharding import PartitionSpec as P

KEY_CHANNELS = 128
DV = 256
BLK = 64


EPS = 1e-06
TAU = 16.0


def rms_norm(values, gain):
    return values * lax.rsqrt(jnp.mean(values * values, axis=-1, keepdims=True) + EPS) * gain


def recurrence(query_proj, key_proj, value_proj, log_decay, head_count):
    seq_rows = query_proj.shape[0]
    blocks = seq_rows // BLK
    exact = lax.Precision.HIGHEST
    queries = query_proj.astype(jnp.float32).reshape(
        blocks, BLK, head_count, KEY_CHANNELS
    ) * KEY_CHANNELS ** (-0.5)
    keys = key_proj.astype(jnp.float32).reshape(blocks, BLK, head_count, KEY_CHANNELS)
    values = value_proj.astype(jnp.float32).reshape(blocks, BLK, head_count, DV)
    decays = log_decay.reshape(blocks, BLK, head_count, KEY_CHANNELS)
    lower = (jnp.arange(BLK)[:, None] >= jnp.arange(BLK)[None, :]).astype(jnp.float32)
    cumul = jnp.einsum("cs,bshd->bchd", lower, decays, precision=exact)
    totals = cumul[:, -1]
    weighted = keys * jnp.exp(totals[:, None] - cumul)
    updates = jnp.einsum("bchd,bche->bhde", weighted, values, precision=exact)
    state = jnp.zeros_like(updates[0])
    previous = []
    for block in range(blocks):
        previous.append(state)
        state = jnp.exp(totals[block])[..., None] * state + updates[block]
    previous = jnp.stack(previous)
    q_decayed = queries * jnp.exp(cumul)
    k_decayed = keys * jnp.exp(-cumul)
    scores = jnp.einsum("bchd,bshd->bhcs", q_decayed, k_decayed, precision=exact)
    scores = scores * lower
    inner = jnp.einsum("bhcs,bshe->bche", scores, values, precision=exact)
    carried = jnp.einsum("bchd,bhde->bche", q_decayed, previous, precision=exact)
    return (inner + carried).reshape(seq_rows, head_count, DV)


def shift(values, axis, distance):
    count = lax.axis_size(axis)
    return lax.ppermute(values, axis, [(i, (i + distance) % count) for i in range(count)])


def swap_core(values):
    return lax.ppermute(values, "tp", [(i, i ^ 1) for i in range(lax.axis_size("tp"))])


def gather_rows(block):
    count = lax.axis_size("tp")
    index = lax.axis_index("tp")
    chips, core, chip = count // 2, index % 2, index // 2
    rows = block.shape[0]
    mine = [block] + [shift(block, "tp", 2 * k) for k in range(1, chips)]
    whole = jnp.zeros((count * rows,) + block.shape[1:], block.dtype)
    for k, piece in enumerate(mine):
        source = (chip - k) % chips
        theirs = swap_core(piece)
        whole = lax.dynamic_update_slice_in_dim(whole, piece, (2 * source + core) * rows, 0)
        whole = lax.dynamic_update_slice_in_dim(whole, theirs, (2 * source + 1 - core) * rows, 0)
    return whole


def scatter_sum(partial):
    count = lax.axis_size("tp")
    index = lax.axis_index("tp")
    chips, core, chip = count // 2, index % 2, index // 2
    rows = partial.shape[0] // count
    blocks = partial.astype(jnp.bfloat16).reshape(chips, 2, rows, partial.shape[1])
    away = lax.dynamic_index_in_dim(blocks, 1 - core, 1, keepdims=False)
    kept = lax.dynamic_index_in_dim(blocks, core, 1, keepdims=False).astype(jnp.float32)
    pair = kept + swap_core(away).astype(jnp.float32)
    rounded = pair.astype(jnp.bfloat16)
    total = lax.dynamic_index_in_dim(pair, chip, 0, keepdims=False)
    for k in range(1, chips):
        outgoing = lax.dynamic_index_in_dim(rounded, (chip + k) % chips, 0, keepdims=False)
        total = total + shift(outgoing, "tp", 2 * k).astype(jnp.float32)
    return total


def row_parts(weight):
    reps = lax.axis_size("rep")
    share = weight.shape[0] // reps
    own = lax.dynamic_slice_in_dim(weight, lax.axis_index("rep") * share, share, 0)
    own = lax.all_gather(own, "fs", axis=0, tiled=True)
    return [own] + [shift(own, "rep", k) for k in range(1, reps)]


def column_parts(weight):
    reps = lax.axis_size("rep")
    share = weight.shape[1] // reps
    own = lax.dynamic_slice_in_dim(weight, lax.axis_index("rep") * share, share, 1)
    own = lax.all_gather(own, "fs", axis=0, tiled=False)
    return [own] + [shift(own, "rep", k) for k in range(1, reps)]


def input_parts(values):
    reps, groups = lax.axis_size("rep"), lax.axis_size("fs")
    share = values.shape[1] // (reps * groups)
    layouts = [
        jnp.concatenate(
            [
                values[:, (g * reps + j) * share : (g * reps + j + 1) * share]
                for g in range(groups)
            ],
            axis=1,
        )
        for j in range(reps)
    ]
    index = lax.axis_index("rep")
    return [
        lax.select_n(jnp.full((), (index - k) % reps, jnp.int32), *layouts) if reps > 2
        else (jnp.where((index - k) % reps == 0, layouts[0], layouts[-1]))
        for k in range(reps)
    ]


def dots(inputs, weights):
    total = jnp.dot(inputs[0], weights[0], preferred_element_type=jnp.float32)
    for left, right in zip(inputs[1:], weights[1:]):
        total = total + jnp.dot(left, right, preferred_element_type=jnp.float32)
    return total


def project_out(values, weights):
    reps = lax.axis_size("rep")
    index = lax.axis_index("rep")
    sums = []
    for weight in weights:
        partial = jnp.concatenate(
            [
                jnp.dot(values, weight[g], preferred_element_type=jnp.float32)
                for g in range(weight.shape[0])
            ],
            axis=1,
        )
        sums.append(scatter_sum(partial))
    share = weights[0].shape[2]
    ordered = []
    for j in range(reps):
        if reps == 2:
            ordered.append(jnp.where(index == j, sums[0], sums[1]))
        else:
            ordered.append(lax.select_n((index - j) % reps, *sums))
    pieces = []
    for g in range(weights[0].shape[0]):
        for j in range(reps):
            pieces.append(ordered[j][:, g * share : (g + 1) * share])
    return jnp.concatenate(pieces, axis=1)


def per_device(
    tokens,
    mix_gain,
    w_query,
    w_key,
    w_value,
    w_decay_down,
    w_decay_up,
    decay_bias,
    decay_shift,
    head_gain,
    w_mix_out,
    ffn_gain,
    w_gate,
    w_up,
    w_down,
):
    tp_index = lax.axis_index("tp")
    key_cols = w_query.shape[1]
    value_cols = w_value.shape[1]
    heads_dev = key_cols // KEY_CHANNELS
    own_tokens = tokens.astype(jnp.float32)
    qkv_weights = row_parts(jnp.concatenate([w_query, w_key, w_value], axis=1))
    out_weights = column_parts(w_mix_out)
    gate_weights = row_parts(w_gate)
    up_weights = row_parts(w_up)
    down_weights = column_parts(w_down)
    normed = gather_rows(rms_norm(own_tokens, mix_gain).astype(jnp.bfloat16))
    seq_rows = normed.shape[0]
    low_rank = jnp.dot(normed, w_decay_down, preferred_element_type=jnp.float32).astype(
        jnp.bfloat16
    )
    up_columns = lax.dynamic_slice_in_dim(w_decay_up, tp_index * key_cols, key_cols, 1)
    bias_columns = lax.dynamic_slice_in_dim(decay_bias, tp_index * key_cols, key_cols, 0)
    pre_decay = jnp.dot(low_rank, up_columns, preferred_element_type=jnp.float32) + bias_columns
    log_decay = jax.nn.log_sigmoid(pre_decay) / TAU + decay_shift
    projected = dots(input_parts(normed), qkv_weights).astype(jnp.bfloat16)
    query_proj = projected[:, :key_cols]
    key_proj = projected[:, key_cols : 2 * key_cols]
    value_proj = projected[:, 2 * key_cols :]
    head_out = recurrence(query_proj, key_proj, value_proj, log_decay, heads_dev)
    gain_columns = lax.dynamic_slice_in_dim(head_gain, tp_index * value_cols, value_cols, 0)
    gated = rms_norm(head_out, gain_columns.reshape(heads_dev, DV)).astype(jnp.bfloat16)
    gated = gated.reshape(seq_rows, value_cols)
    hidden = own_tokens + project_out(gated, out_weights)
    normed_ffn = gather_rows(rms_norm(hidden, ffn_gain).astype(jnp.bfloat16))
    ffn_inputs = input_parts(normed_ffn)
    gate_proj = dots(ffn_inputs, gate_weights)
    up_proj = dots(ffn_inputs, up_weights)
    activated = (jax.nn.silu(gate_proj) * up_proj).astype(jnp.bfloat16)
    return hidden + project_out(activated, down_weights)


BF16 = jnp.bfloat16
F32 = jnp.float32
MESH_ID = pl.DeviceIdType.MESH
KINDS = ("end_a", "end_b", "mid_own", "mid_end", "rep_own", "rep_end")
PARTS = ("qkv0", "qkv1", "out", "gate0", "up0", "gate1", "up1", "down0", "down1", "down2", "down3")
DOWN = PARTS[-4:]


def layer_kernel(
    tokens, mix_gain, w_query, w_key, w_value, w_decay_down, w_decay_up, decay_bias,
    decay_shift, head_gain, w_mix_out, ffn_gain, w_gate, w_up, w_down,
    out,
    wq, wo, wg, wu, wd, tok, shift, x_mix, x_ffn, proj, gated, part, near, far, near2, far2,
    act, hid, mixed_home, ffn_home, state, shift_sent,
    load_sem, w_send, w_recv, a_send, a_recv,
):
    r, z, t = lax.axis_index("rep"), lax.axis_index("fs"), lax.axis_index("tp")
    depth, key_cols = w_query.shape
    value_cols = w_value.shape[1]
    rows, width = tokens.shape
    seq = rows * 4
    hidden_units = w_gate.shape[1]
    block = width // 8
    half_rows = depth // 2
    cut = (hidden_units // 256 + 1) // 2 * 256
    heads = key_cols // KEY_CHANNELS
    zc = 1 + z // 2
    ze = 3 * (z // 2)
    zo, zf = 3 - zc, 3 - ze
    other_r = 1 - r
    core = t + 1 - 2 * lax.rem(t, 2)
    chip = lax.rem(t + 2, 4)
    both = 3 - t
    pair_z = z + 1 - 2 * lax.rem(z, 2)
    is_centre = jnp.logical_and(z >= 1, z <= 2)

    barrier = pltpu.get_barrier_semaphore()
    for partner in ({"fs": pair_z}, {"fs": 3 - z}, {"rep": other_r}, {"tp": core}, {"tp": chip}):
        pl.semaphore_signal(barrier, inc=1, device_id=partner, device_id_type=MESH_ID)

    def region(name, plane, half):
        at = pl.multiple_of(plane * depth + half * half_rows, half_rows)
        if name.startswith("qkv"):
            piece = half_rows // 2
            return wq.at[pl.ds(pl.multiple_of(at + int(name[-1]) * piece, piece), piece), :]
        if name == "out":
            return wo.at[2 * plane + half]
        if name.startswith("down"):
            piece = hidden_units // 4
            return wd.at[2 * plane + half, pl.ds(int(name[-1]) * piece, piece)]
        ref = wg if name.startswith("gate") else wu
        if name.endswith("0"):
            return ref.at[pl.ds(at, half_rows), pl.ds(0, cut)]
        return ref.at[pl.ds(at, half_rows), pl.ds(cut, hidden_units - cut)]

    def weight_copy(name, kind, plane, half, device):
        ref = region(name, plane, half)
        index = PARTS.index(name) * len(KINDS) + KINDS.index(kind)
        return pltpu.make_async_remote_copy(
            src_ref=ref, dst_ref=ref, send_sem=w_send.at[index], recv_sem=w_recv.at[index],
            device_id=device, device_id_type=MESH_ID,
        )

    act_ids = {}

    def act_copy(key, src, dst, device):
        index = act_ids.setdefault(key, len(act_ids))
        return pltpu.make_async_remote_copy(
            src_ref=src, dst_ref=dst, send_sem=a_send.at[index], recv_sem=a_recv.at[index],
            device_id=device, device_id_type=MESH_ID,
        )

    at_z = pl.multiple_of(z * depth, depth)
    loads = {}

    def load(name, src, dst):
        copy = pltpu.make_async_copy(src, dst, load_sem.at[len(loads)])
        copy.start()
        loads[name] = copy

    load("q", w_query, wq.at[pl.ds(at_z, depth), pl.ds(0, key_cols)])
    load("k", w_key, wq.at[pl.ds(at_z, depth), pl.ds(key_cols, key_cols)])
    load("v", w_value, wq.at[pl.ds(at_z, depth), pl.ds(2 * key_cols, value_cols)])
    load("tok", tokens, tok.at[0])
    load("o0", w_mix_out.at[:, pl.ds(0, block)], wo.at[2 * z])
    load("o1", w_mix_out.at[:, pl.ds(block, block)], wo.at[2 * z + 1])
    load("shift", decay_shift, shift.at[0])
    load("g", w_gate, wg.at[pl.ds(at_z, depth), :])
    load("u", w_up, wu.at[pl.ds(at_z, depth), :])
    load("d0", w_down.at[:, pl.ds(0, block)], wd.at[2 * z])
    load("d1", w_down.at[:, pl.ds(block, block)], wd.at[2 * z + 1])
    pl.semaphore_wait(barrier, 5)
    for name in ("q", "k", "v"):
        loads[name].wait()

    tok_copy = act_copy("tok", tok.at[0], tok.at[1], {"fs": pair_z})
    shift_copy = act_copy("shift", shift_sent.at[0], shift_sent.at[1], {"fs": pair_z})

    out_order = [
        (2 * zc, None), (2 * zc + 1, None),
        (2 * zo + r, ("mid_own", zo, r)), (2 * ze + r, ("end_a", ze, r)),
        (2 * zo + other_r, ("rep_own", zo, other_r)), (2 * zf + r, ("mid_end", zf, r)),
        (2 * ze + other_r, ("end_b", ze, other_r)), (2 * zf + other_r, ("rep_end", zf, other_r)),
    ]
    mixed_copy = act_copy("mixed", mixed_home, mixed_home, {"fs": pair_z})
    home_copies = [
        act_copy(("home", i), ffn_home.at[b], ffn_home.at[b], {"fs": pair_z})
        for i, (b, _) in enumerate(out_order)
    ]

    @pl.when(jnp.logical_not(is_centre))
    def _():
        sent = []

        def send(name, kind, half):
            copy = weight_copy(name, kind, z, half, {"fs": pair_z})
            copy.start()
            sent.append(copy)

        send("qkv0", "end_a", r)
        send("qkv1", "end_a", r)
        loads["o0"].wait()
        loads["o1"].wait()
        send("out", "end_a", r)
        loads["tok"].wait()
        tok_copy.start()
        send("qkv0", "end_b", other_r)
        loads["shift"].wait()
        shift_sent[0] = shift[0].astype(BF16)
        shift_copy.start()
        send("out", "end_b", other_r)
        for name in ("g", "u", "d0", "d1"):
            loads[name].wait()
        for name in ("gate0", "up0", "gate1", "up1"):
            send(name, "end_a", r)
        for name in ("gate0", "up0", "gate1", "up1"):
            send(name, "end_b", other_r)
        for name in DOWN:
            send(name, "end_a", r)
        for name in DOWN:
            send(name, "end_b", other_r)
        mixed_copy.wait_recv()
        for i, (b, _) in enumerate(out_order):
            home_copies[i].wait_recv()
            cols = pl.ds(pl.multiple_of(b * block, block), block)
            out[:, cols] = mixed_home[b].astype(F32) + ffn_home[b].astype(F32)
        tok_copy.wait_send()
        shift_copy.wait_send()
        for copy in sent:
            copy.wait_send()

    @pl.when(is_centre)
    def _():
        sent = []

        arrived = set()

        def incoming(name, kind, plane, half):
            if (name, kind) not in arrived:
                arrived.add((name, kind))
                weight_copy(name, kind, plane, half, {"fs": pair_z}).wait_recv()

        def send(name, kind, plane, half, device):
            copy = weight_copy(name, kind, plane, half, device)
            copy.start()
            sent.append(copy)

        def mid_own(*parts):
            for name in parts:
                send(name, "mid_own", z, r, {"fs": zo})

        def mid_end(*parts):
            for name in parts:
                incoming(name, "end_a", ze, r)
                send(name, "mid_end", ze, r, {"fs": zo})

        def rep_own(*parts):
            for name in parts:
                incoming(name, "mid_own", zo, r)
                send(name, "rep_own", zo, r, {"rep": other_r})

        def rep_end(*parts):
            for name in parts:
                incoming(name, "mid_end", zf, r)
                send(name, "rep_end", zf, r, {"rep": other_r})

        def rep_end_b(*parts):
            for name in parts:
                incoming(name, "end_a", ze, r)
                send(name, "end_b", ze, r, {"rep": other_r})

        def mid_own_b(*parts):
            for name in parts:
                send(name, "rep_own", z, other_r, {"fs": zo})

        def complete(*parts):
            for name in parts:
                incoming(name, "mid_own", zo, r)
                incoming(name, "end_b", ze, other_r)
                incoming(name, "rep_own", zo, other_r)
                incoming(name, "rep_end", zf, other_r)

        def norm_rows(load_rows, gain, dst, s):
            @pl.loop(0, rows // 16)
            def _(i):
                values = load_rows(pl.ds(pl.multiple_of(i * 16, 16), 16))
                scale = lax.rsqrt(jnp.mean(values * values, axis=-1, keepdims=True) + EPS)
                at = pl.multiple_of(t * rows + i * 16, 16)
                dst[s, pl.ds(at, 16), :] = (values * scale * gain[...]).astype(BF16)

        class Gather:
            def __init__(self, key, ref, s):
                def rows_of(device):
                    return ref.at[s, pl.ds(pl.multiple_of(device * rows, rows), rows), :]

                mine, theirs = rows_of(t), rows_of(chip)
                self.to_chip = act_copy((key, s, "chip"), mine, mine, {"tp": chip})
                self.to_core = act_copy((key, s, "core"), mine, mine, {"tp": core})
                self.pass_on = act_copy((key, s, "pass"), theirs, theirs, {"tp": core})
                self.from_chip = act_copy((key, s, "chip"), theirs, theirs, {"tp": chip})
                self.from_core = act_copy((key, s, "core"), rows_of(core), rows_of(core), {"tp": core})
                self.passed = act_copy((key, s, "pass"), rows_of(both), rows_of(both), {"tp": core})

            def start(self):
                self.to_chip.start()
                self.to_core.start()

            def forward(self):
                self.from_chip.wait_recv()
                self.pass_on.start()

            def finish(self):
                self.from_core.wait_recv()
                self.passed.wait_recv()

            def drain(self):
                self.to_chip.wait_send()
                self.to_core.wait_send()
                self.pass_on.wait_send()

        mid_own("qkv0", "qkv1")
        loads["tok"].wait()
        norm_rows(lambda at: tok[0, at, :].astype(F32), mix_gain, x_mix, 0)
        mix_gather = [Gather("mix", x_mix, s) for s in range(2)]
        ffn_gather = [Gather("ffn", x_ffn, s) for s in range(2)]
        mix_gather[0].start()
        for name in ("o0", "o1", "shift", "g", "u", "d0", "d1"):
            loads[name].wait()
        bias = decay_bias[:, pl.ds(pl.multiple_of(t * key_cols, key_cols), key_cols)]
        up_cols = w_decay_up[:, pl.ds(pl.multiple_of(t * key_cols, key_cols), key_cols)]

        def project(s):
            @pl.loop(0, seq // 256)
            def _(i):
                at = pl.ds(pl.multiple_of(i * 256, 256), 256)
                x = x_mix[s, at, :]
                for n in range(0, 2 * key_cols + value_cols, 512):
                    cols = pl.ds(n, 512)
                    proj[s, at, cols] = jnp.dot(x, wq[:, cols], preferred_element_type=F32).astype(BF16)
                low = lax.dot_general(
                    x, w_decay_down[...], (((1,), (1,)), ((), ())), preferred_element_type=F32
                ).astype(BF16)
                pre = jnp.dot(low, up_cols, preferred_element_type=F32) + bias
                log_sig = jnp.minimum(pre, 0.0) - jnp.log1p(jnp.exp(-jnp.abs(pre)))
                given = shift[0, at, :] if s == 0 else shift_sent[1, at, :].astype(F32)
                shift[s, at, :] = log_sig / TAU + given

        lower = (
            lax.broadcasted_iota(jnp.int32, (BLK, BLK), 0) >= lax.broadcasted_iota(jnp.int32, (BLK, BLK), 1)
        )
        gain_cols = head_gain[:, pl.ds(pl.multiple_of(t * value_cols, value_cols), value_cols)]

        def attend(s, lo, hi):
            if lo == 0:
                state[...] = jnp.zeros_like(state)

            @pl.loop(lo, hi)
            def _(b):
                at = pl.ds(pl.multiple_of(b * BLK, BLK), BLK)
                for h in range(heads):
                    key_at = pl.ds(h * KEY_CHANNELS, KEY_CHANNELS)
                    decays = shift[s, at, key_at]
                    cumul = jnp.dot(
                        lower.astype(F32), decays, precision=lax.Precision.HIGHEST,
                        preferred_element_type=F32,
                    )
                    total = cumul[BLK - 1 :, :]
                    queries = proj[s, at, key_at].astype(F32) * KEY_CHANNELS ** (-0.5)
                    keys = proj[s, at, pl.ds(key_cols + h * KEY_CHANNELS, KEY_CHANNELS)].astype(F32)
                    values = proj[s, at, pl.ds(2 * key_cols + h * DV, DV)]
                    q_decayed = (queries * jnp.exp(cumul)).astype(BF16)
                    k_decayed = (keys * jnp.exp(-cumul)).astype(BF16)
                    weighted = (keys * jnp.exp(total - cumul)).astype(BF16)
                    scores = lax.dot_general(
                        q_decayed, k_decayed, (((1,), (1,)), ((), ())), preferred_element_type=F32
                    )
                    scores = jnp.where(lower, scores, 0.0).astype(BF16)
                    before = state[h]
                    result = jnp.dot(scores, values, preferred_element_type=F32) + lax.dot_general(
                        q_decayed, before.astype(BF16), (((1,), (1,)), ((), ())), preferred_element_type=F32
                    )
                    state[h] = jnp.exp(total) * before + lax.dot_general(
                        values, weighted, (((0,), (0,)), ((), ())), preferred_element_type=F32
                    )
                    scale = lax.rsqrt(jnp.mean(result * result, axis=-1, keepdims=True) + EPS)
                    gated[s, at, pl.ds(h * DV, DV)] = (
                        result * scale * gain_cols[:, h * DV : (h + 1) * DV]
                    ).astype(BF16)

        def mix_out(s):
            @pl.loop(0, 8)
            def _(b):
                value = jnp.dot(gated[s], wo[b], preferred_element_type=F32).astype(BF16)
                for k in range(4):
                    part[b, k, s] = value[k * rows : (k + 1) * rows]

        def reduce_copies(s):
            return (
                act_copy(("red", s, 0), part.at[:, core, s], near.at[0, s], {"tp": core}),
                act_copy(("red", s, 1), part.at[:, both, s], near.at[1, s], {"tp": core}),
                act_copy(("red", s, 2), part.at[:, chip, s], far.at[s], {"tp": chip}),
            )

        reduce = [reduce_copies(s) for s in range(2)]

        def reduce_far(s):
            reduce[s][1].wait_recv()

            @pl.loop(0, 8)
            def _(b):
                total = part[b, chip, s].astype(F32) + near[1, s, b].astype(F32)
                part[b, chip, s] = total.astype(BF16)

            reduce[s][2].start()

        def reduce_end(s):
            reduce[s][0].wait_recv()
            reduce[s][2].wait_recv()
            for b in range(8):
                cols = pl.ds(b * block, block)
                total = part[b, t, s].astype(F32) + near[0, s, b].astype(F32) + far[s, b].astype(F32)
                hid[s, :, cols] = tok[s, :, cols].astype(F32) + total
                if s == 1:
                    mixed_home[b] = total.astype(BF16)
                else:
                    out[:, cols] = total
            if s == 1:
                mixed_copy.start()
            norm_rows(lambda at: hid[s, at, :], ffn_gain, x_ffn, s)
            ffn_gather[s].start()

        def expand(s, lo, hi):
            @pl.loop(0, seq // 256)
            def _(i):
                at = pl.ds(pl.multiple_of(i * 256, 256), 256)
                x = x_ffn[s, at, :]
                for n in range(lo, hi, 256):
                    cols = pl.ds(n, min(256, hi - n))
                    gate = jnp.dot(x, wg[:, cols], preferred_element_type=F32)
                    up = jnp.dot(x, wu[:, cols], preferred_element_type=F32)
                    act[s, at, cols] = (gate / (1.0 + jnp.exp(-gate)) * up).astype(BF16)

        def piece_copies(i, b):
            return (
                act_copy(("piece", i, 0), part.at[b, core], near2.at[i, 0], {"tp": core}),
                act_copy(("piece", i, 1), part.at[b, both], near2.at[i, 1], {"tp": core}),
                act_copy(("piece", i, 2), part.at[b, chip], far2.at[i], {"tp": chip}),
            )

        pieces = [piece_copies(i, b) for i, (b, _) in enumerate(out_order)]

        def reduce_start(s):
            reduce[s][1].start()
            reduce[s][0].start()

        def reduce_drain():
            for s in range(2):
                for copy in reduce[s]:
                    copy.wait_send()

        def piece_dot(i):
            b, source = out_order[i]
            if source is not None:
                for name in DOWN:
                    incoming(name, *source)
            for s in range(2):
                value = jnp.dot(act[s], wd[b], preferred_element_type=F32).astype(BF16)
                for k in range(4):
                    part[b, k, s] = value[k * rows : (k + 1) * rows]
            pieces[i][1].start()
            pieces[i][0].start()

        def piece_far(i):
            b = out_order[i][0]
            pieces[i][1].wait_recv()
            part[b, chip] = (part[b, chip].astype(F32) + near2[i, 1].astype(F32)).astype(BF16)
            pieces[i][2].start()

        def piece_end(i):
            b = out_order[i][0]
            pieces[i][0].wait_recv()
            pieces[i][2].wait_recv()
            total = part[b, t].astype(F32) + near2[i, 0].astype(F32) + far2[i].astype(F32)
            cols = pl.ds(pl.multiple_of(b * block, block), block)
            ffn_home[b] = total[1].astype(BF16)
            home_copies[i].start()
            out[:, cols] = out[:, cols] + total[0]

        n_blk = seq // BLK
        mid_end("qkv0")
        rep_own("qkv0")
        mid_end("qkv1")
        rep_own("qkv1")
        rep_end_b("qkv1")
        mid_own("out")
        mix_gather[0].forward()
        mid_end("out")
        mid_own("gate0", "up0")
        rep_end("qkv0")
        rep_end("qkv1")
        rep_own("out")
        mix_gather[0].finish()
        tok_copy.wait_recv()
        norm_rows(lambda at: tok[1, at, :].astype(F32), mix_gain, x_mix, 1)
        mix_gather[1].start()
        rep_end("out")
        mid_own("gate1")
        complete("qkv0", "qkv1")
        project(0)
        attend(0, 0, n_blk // 2)
        rep_own("gate0")
        mix_gather[1].forward()
        attend(0, n_blk // 2, n_blk)
        complete("out")
        mix_out(0)
        reduce_start(0)
        mix_gather[1].finish()
        shift_copy.wait_recv()
        project(1)
        reduce_far(0)
        rep_own("up0")
        attend(1, 0, n_blk // 2)
        mid_end("gate0")
        rep_own("gate1")
        attend(1, n_blk // 2, n_blk)
        mix_out(1)
        reduce_start(1)
        mid_end("up0")
        mid_own("up1")
        reduce_far(1)
        rep_end("gate0")
        reduce_end(0)
        mid_end("gate1")
        rep_end("up0")
        mid_end("up1")
        reduce_end(1)
        mid_own(*DOWN)
        rep_own("up1")
        ffn_gather[0].forward()
        rep_end("gate1")
        complete("gate0", "up0")
        ffn_gather[0].finish()
        rep_end("up1")
        expand(0, 0, cut)
        ffn_gather[1].forward()
        rep_own("down0")
        ffn_gather[1].finish()
        expand(1, 0, cut)
        rep_own("down1")
        complete("gate1", "up1")
        rep_own("down2")
        expand(0, cut, hidden_units)
        rep_own("down3")
        mid_end("down0")
        expand(1, cut, hidden_units)
        mid_end("down1")
        reduce_drain()
        piece_dot(0)
        piece_dot(1)
        piece_far(0)
        mid_end("down2")
        rep_end("down0")
        piece_dot(2)
        piece_far(1)
        mid_end("down3")
        piece_dot(3)
        piece_far(2)
        piece_end(0)
        rep_end("down1")
        piece_dot(4)
        piece_far(3)
        piece_end(1)
        rep_end("down2")
        piece_far(4)
        piece_end(2)
        rep_end("down3")
        piece_dot(5)
        piece_end(3)
        piece_far(5)
        piece_end(4)
        piece_dot(6)
        piece_far(6)
        piece_end(5)
        piece_dot(7)
        piece_far(7)
        piece_end(6)
        piece_end(7)
        for gather in mix_gather + ffn_gather:
            gather.drain()
        for copies in pieces:
            for copy in copies:
                copy.wait_send()
        mixed_copy.wait_send()
        for copy in home_copies:
            copy.wait_send()
        for copy in sent:
            copy.wait_send()


def per_device_kernel(
    tokens, mix_gain, w_query, w_key, w_value, w_decay_down, w_decay_up, decay_bias,
    decay_shift, head_gain, w_mix_out, ffn_gain, w_gate, w_up, w_down,
):
    rows, width = tokens.shape
    planes, tps = lax.axis_size("fs"), lax.axis_size("tp")
    key_cols, value_cols, hidden_units = w_query.shape[1], w_value.shape[1], w_gate.shape[1]
    depth = w_query.shape[0]
    seq = rows * tps
    blocks = 2 * planes
    block = width // blocks
    any_spec = pl.BlockSpec(memory_space=pl.ANY)
    vmem_spec = pl.BlockSpec(memory_space=pltpu.VMEM)
    large = {0, 2, 3, 4, 8, 10, 12, 13, 14}
    args = (
        tokens, mix_gain.reshape(1, -1), w_query, w_key, w_value, w_decay_down.T, w_decay_up,
        decay_bias.reshape(1, -1), decay_shift, head_gain.reshape(1, -1), w_mix_out,
        ffn_gain.reshape(1, -1), w_gate, w_up, w_down,
    )
    delta = pl.pallas_call(
        layer_kernel,
        out_shape=jax.ShapeDtypeStruct((rows, width), F32),
        in_specs=[any_spec if i in large else vmem_spec for i in range(len(args))],
        out_specs=vmem_spec,
        scratch_shapes=[
            pltpu.VMEM((planes * depth, 2 * key_cols + value_cols), BF16),
            pltpu.VMEM((blocks, value_cols, block), BF16),
            pltpu.VMEM((planes * depth, hidden_units), BF16),
            pltpu.VMEM((planes * depth, hidden_units), BF16),
            pltpu.VMEM((blocks, hidden_units, block), BF16),
            pltpu.VMEM((2, rows, width), BF16),
            pltpu.VMEM((2, seq, key_cols), F32),
            pltpu.VMEM((2, seq, width), BF16),
            pltpu.VMEM((2, seq, width), BF16),
            pltpu.VMEM((2, seq, 2 * key_cols + value_cols), BF16),
            pltpu.VMEM((2, seq, value_cols), BF16),
            pltpu.VMEM((blocks, tps, 2, rows, block), BF16),
            pltpu.VMEM((2, 2, blocks, rows, block), BF16),
            pltpu.VMEM((2, blocks, rows, block), BF16),
            pltpu.VMEM((blocks, 2, 2, rows, block), BF16),
            pltpu.VMEM((blocks, 2, rows, block), BF16),
            pltpu.VMEM((2, seq, hidden_units), BF16),
            pltpu.VMEM((2, rows, width), F32),
            pltpu.VMEM((blocks, rows, block), BF16),
            pltpu.VMEM((blocks, rows, block), BF16),
            pltpu.VMEM((key_cols // KEY_CHANNELS, DV, KEY_CHANNELS), F32),
            pltpu.VMEM((2, seq, key_cols), BF16),
            pltpu.SemaphoreType.DMA((16,)),
            pltpu.SemaphoreType.DMA((len(PARTS) * len(KINDS),)),
            pltpu.SemaphoreType.DMA((len(PARTS) * len(KINDS),)),
            pltpu.SemaphoreType.DMA((64,)),
            pltpu.SemaphoreType.DMA((64,)),
        ],
        compiler_params=pltpu.CompilerParams(
            collective_id=0, has_side_effects=True, vmem_limit_bytes=67043328
        ),
    )(*args)
    return tokens.astype(F32) + delta


def solution(mesh):
    shape = dict(mesh.shape)
    small = shape["rep"] == 2 and shape["fs"] == 4 and shape["tp"] == 4
    return jax.shard_map(
        per_device_kernel if small else per_device,
        mesh=mesh,
        in_specs=(
            P(("rep", "fs", "tp"), None),
            P(),
            P("fs", "tp"),
            P("fs", "tp"),
            P("fs", "tp"),
            P(),
            P(),
            P(),
            P(("rep", "fs"), "tp"),
            P(),
            P("tp", "fs"),
            P(),
            P("fs", "tp"),
            P("fs", "tp"),
            P("tp", "fs"),
        ),
        out_specs=P(("rep", "fs", "tp"), None),
        check_vma=False,
    )
```

```python
import math

import jax
import jax.numpy as jnp
from jax import lax
from jax.experimental import pallas as pl
from jax.experimental.pallas import tpu as pltpu
from jax.sharding import PartitionSpec as P

KEY_CHANNELS = 128
DV = 256
BLK = 64


EPS = 1e-06
TAU = 16.0


def rms_norm(values, gain):
    return values * lax.rsqrt(jnp.mean(values * values, axis=-1, keepdims=True) + EPS) * gain


def recurrence(query_proj, key_proj, value_proj, log_decay, head_count):
    seq_rows = query_proj.shape[0]
    blocks = seq_rows // BLK
    exact = lax.Precision.HIGHEST
    queries = query_proj.astype(jnp.float32).reshape(
        blocks, BLK, head_count, KEY_CHANNELS
    ) * KEY_CHANNELS ** (-0.5)
    keys = key_proj.astype(jnp.float32).reshape(blocks, BLK, head_count, KEY_CHANNELS)
    values = value_proj.astype(jnp.float32).reshape(blocks, BLK, head_count, DV)
    decays = log_decay.reshape(blocks, BLK, head_count, KEY_CHANNELS)
    lower = (jnp.arange(BLK)[:, None] >= jnp.arange(BLK)[None, :]).astype(jnp.float32)
    cumul = jnp.einsum("cs,bshd->bchd", lower, decays, precision=exact)
    totals = cumul[:, -1]
    weighted = keys * jnp.exp(totals[:, None] - cumul)
    updates = jnp.einsum("bchd,bche->bhde", weighted, values, precision=exact)
    state = jnp.zeros_like(updates[0])
    previous = []
    for block in range(blocks):
        previous.append(state)
        state = jnp.exp(totals[block])[..., None] * state + updates[block]
    previous = jnp.stack(previous)
    q_decayed = queries * jnp.exp(cumul)
    k_decayed = keys * jnp.exp(-cumul)
    scores = jnp.einsum("bchd,bshd->bhcs", q_decayed, k_decayed, precision=exact)
    scores = scores * lower
    inner = jnp.einsum("bhcs,bshe->bche", scores, values, precision=exact)
    carried = jnp.einsum("bchd,bhde->bche", q_decayed, previous, precision=exact)
    return (inner + carried).reshape(seq_rows, head_count, DV)


def shift(values, axis, distance):
    count = lax.axis_size(axis)
    return lax.ppermute(values, axis, [(i, (i + distance) % count) for i in range(count)])


def swap_core(values):
    return lax.ppermute(values, "tp", [(i, i ^ 1) for i in range(lax.axis_size("tp"))])


def gather_rows(block):
    count = lax.axis_size("tp")
    index = lax.axis_index("tp")
    chips, core, chip = count // 2, index % 2, index // 2
    rows = block.shape[0]
    mine = [block] + [shift(block, "tp", 2 * k) for k in range(1, chips)]
    whole = jnp.zeros((count * rows,) + block.shape[1:], block.dtype)
    for k, piece in enumerate(mine):
        source = (chip - k) % chips
        theirs = swap_core(piece)
        whole = lax.dynamic_update_slice_in_dim(whole, piece, (2 * source + core) * rows, 0)
        whole = lax.dynamic_update_slice_in_dim(whole, theirs, (2 * source + 1 - core) * rows, 0)
    return whole


def scatter_sum(partial):
    count = lax.axis_size("tp")
    index = lax.axis_index("tp")
    chips, core, chip = count // 2, index % 2, index // 2
    rows = partial.shape[0] // count
    blocks = partial.astype(jnp.bfloat16).reshape(chips, 2, rows, partial.shape[1])
    away = lax.dynamic_index_in_dim(blocks, 1 - core, 1, keepdims=False)
    kept = lax.dynamic_index_in_dim(blocks, core, 1, keepdims=False).astype(jnp.float32)
    pair = kept + swap_core(away).astype(jnp.float32)
    rounded = pair.astype(jnp.bfloat16)
    total = lax.dynamic_index_in_dim(pair, chip, 0, keepdims=False)
    for k in range(1, chips):
        outgoing = lax.dynamic_index_in_dim(rounded, (chip + k) % chips, 0, keepdims=False)
        total = total + shift(outgoing, "tp", 2 * k).astype(jnp.float32)
    return total


def row_parts(weight):
    reps = lax.axis_size("rep")
    share = weight.shape[0] // reps
    own = lax.dynamic_slice_in_dim(weight, lax.axis_index("rep") * share, share, 0)
    own = lax.all_gather(own, "fs", axis=0, tiled=True)
    return [own] + [shift(own, "rep", k) for k in range(1, reps)]


def column_parts(weight):
    reps = lax.axis_size("rep")
    share = weight.shape[1] // reps
    own = lax.dynamic_slice_in_dim(weight, lax.axis_index("rep") * share, share, 1)
    own = lax.all_gather(own, "fs", axis=0, tiled=False)
    return [own] + [shift(own, "rep", k) for k in range(1, reps)]


def input_parts(values):
    reps, groups = lax.axis_size("rep"), lax.axis_size("fs")
    share = values.shape[1] // (reps * groups)
    layouts = [
        jnp.concatenate(
            [
                values[:, (g * reps + j) * share : (g * reps + j + 1) * share]
                for g in range(groups)
            ],
            axis=1,
        )
        for j in range(reps)
    ]
    index = lax.axis_index("rep")
    return [
        lax.select_n(jnp.full((), (index - k) % reps, jnp.int32), *layouts) if reps > 2
        else (jnp.where((index - k) % reps == 0, layouts[0], layouts[-1]))
        for k in range(reps)
    ]


def dots(inputs, weights):
    total = jnp.dot(inputs[0], weights[0], preferred_element_type=jnp.float32)
    for left, right in zip(inputs[1:], weights[1:]):
        total = total + jnp.dot(left, right, preferred_element_type=jnp.float32)
    return total


def project_out(values, weights):
    reps = lax.axis_size("rep")
    index = lax.axis_index("rep")
    sums = []
    for weight in weights:
        partial = jnp.concatenate(
            [
                jnp.dot(values, weight[g], preferred_element_type=jnp.float32)
                for g in range(weight.shape[0])
            ],
            axis=1,
        )
        sums.append(scatter_sum(partial))
    share = weights[0].shape[2]
    ordered = []
    for j in range(reps):
        if reps == 2:
            ordered.append(jnp.where(index == j, sums[0], sums[1]))
        else:
            ordered.append(lax.select_n((index - j) % reps, *sums))
    pieces = []
    for g in range(weights[0].shape[0]):
        for j in range(reps):
            pieces.append(ordered[j][:, g * share : (g + 1) * share])
    return jnp.concatenate(pieces, axis=1)


def per_device(
    tokens,
    mix_gain,
    w_query,
    w_key,
    w_value,
    w_decay_down,
    w_decay_up,
    decay_bias,
    decay_shift,
    head_gain,
    w_mix_out,
    ffn_gain,
    w_gate,
    w_up,
    w_down,
):
    tp_index = lax.axis_index("tp")
    key_cols = w_query.shape[1]
    value_cols = w_value.shape[1]
    heads_dev = key_cols // KEY_CHANNELS
    own_tokens = tokens.astype(jnp.float32)
    qkv_weights = row_parts(jnp.concatenate([w_query, w_key, w_value], axis=1))
    out_weights = column_parts(w_mix_out)
    gate_weights = row_parts(w_gate)
    up_weights = row_parts(w_up)
    down_weights = column_parts(w_down)
    normed = gather_rows(rms_norm(own_tokens, mix_gain).astype(jnp.bfloat16))
    seq_rows = normed.shape[0]
    low_rank = jnp.dot(normed, w_decay_down, preferred_element_type=jnp.float32).astype(
        jnp.bfloat16
    )
    up_columns = lax.dynamic_slice_in_dim(w_decay_up, tp_index * key_cols, key_cols, 1)
    bias_columns = lax.dynamic_slice_in_dim(decay_bias, tp_index * key_cols, key_cols, 0)
    pre_decay = jnp.dot(low_rank, up_columns, preferred_element_type=jnp.float32) + bias_columns
    log_decay = jax.nn.log_sigmoid(pre_decay) / TAU + decay_shift
    projected = dots(input_parts(normed), qkv_weights).astype(jnp.bfloat16)
    query_proj = projected[:, :key_cols]
    key_proj = projected[:, key_cols : 2 * key_cols]
    value_proj = projected[:, 2 * key_cols :]
    head_out = recurrence(query_proj, key_proj, value_proj, log_decay, heads_dev)
    gain_columns = lax.dynamic_slice_in_dim(head_gain, tp_index * value_cols, value_cols, 0)
    gated = rms_norm(head_out, gain_columns.reshape(heads_dev, DV)).astype(jnp.bfloat16)
    gated = gated.reshape(seq_rows, value_cols)
    hidden = own_tokens + project_out(gated, out_weights)
    normed_ffn = gather_rows(rms_norm(hidden, ffn_gain).astype(jnp.bfloat16))
    ffn_inputs = input_parts(normed_ffn)
    gate_proj = dots(ffn_inputs, gate_weights)
    up_proj = dots(ffn_inputs, up_weights)
    activated = (jax.nn.silu(gate_proj) * up_proj).astype(jnp.bfloat16)
    return hidden + project_out(activated, down_weights)


BF16 = jnp.bfloat16
F32 = jnp.float32
MESH_ID = pl.DeviceIdType.MESH
KINDS = ("end_a", "end_b", "mid_own", "mid_end", "rep_own", "rep_end")
PARTS = ("qkv0", "qkv1", "qkv2", "qkv3", "out", "gate0", "up0", "gate1", "up1", "down0", "down1", "down2", "down3")
DOWN = PARTS[-4:]
GROUPS = {"mix": 0, "ffn": 1, "piece": 2, "home": 2, "mixed": 2, "red": 3, "tok": 4, "shift": 5}
QKV = PARTS[:4]


def layer_kernel(
    tokens, mix_gain, w_query, w_key, w_value, w_decay_down, w_decay_up, decay_bias,
    decay_shift, head_gain, w_mix_out, ffn_gain, w_gate, w_up, w_down,
    out,
    wq, wo, wg, wu, wd, tok, shift, x_mix, x_ffn, proj, gated, part, near, far, near2, far2,
    act, hid, mixed_home, ffn_home, state, shift_sent, early,
    load_sem, w_send, w_recv, a_send, a_recv,
):
    r, z, t = lax.axis_index("rep"), lax.axis_index("fs"), lax.axis_index("tp")
    depth, key_cols = w_query.shape
    value_cols = w_value.shape[1]
    rows, width = tokens.shape
    seq = rows * 4
    hidden_units = w_gate.shape[1]
    block = width // 8
    half_rows = depth // 2
    cut = (hidden_units // 256 + 1) // 2 * 256
    down_rows = (hidden_units // 2 + 127) // 128 * 128
    lane = block // 2
    heads = key_cols // KEY_CHANNELS
    zc = 1 + z // 2
    ze = 3 * (z // 2)
    zo, zf = 3 - zc, 3 - ze
    other_r = 1 - r
    core = t + 1 - 2 * lax.rem(t, 2)
    chip = lax.rem(t + 2, 4)
    both = 3 - t
    pair_z = z + 1 - 2 * lax.rem(z, 2)
    is_centre = jnp.logical_and(z >= 1, z <= 2)

    barrier = pltpu.get_barrier_semaphore()
    for partner in (
        {"fs": pair_z}, {"fs": 3 - z}, {"rep": other_r}, {"tp": core}, {"tp": chip},
        {"fs": pair_z, "tp": chip},
    ):
        pl.semaphore_signal(barrier, inc=1, device_id=partner, device_id_type=MESH_ID)

    def region(name, plane, half):
        at = pl.multiple_of(plane * depth + half * half_rows, half_rows)
        if name.startswith("qkv"):
            piece = half_rows // 4
            return wq.at[pl.ds(pl.multiple_of(at + int(name[-1]) * piece, piece), piece), :]
        if name == "out":
            return wo.at[2 * plane + half]
        if name.startswith("down"):
            lanes, part_at = divmod(int(name[-1]), 2)
            lo = part_at * down_rows
            return wd.at[
                2 * plane + half, pl.ds(lo, min(down_rows, hidden_units - lo)), pl.ds(lanes * lane, lane)
            ]
        ref = wg if name.startswith("gate") else wu
        if name.endswith("0"):
            return ref.at[pl.ds(at, half_rows), pl.ds(0, cut)]
        return ref.at[pl.ds(at, half_rows), pl.ds(cut, hidden_units - cut)]

    def weight_copy(name, kind, plane, half, device):
        ref = region(name, plane, half)
        index = PARTS.index(name) * len(KINDS) + KINDS.index(kind)
        return pltpu.make_async_remote_copy(
            src_ref=ref, dst_ref=ref, send_sem=w_send.at[KINDS.index(kind)], recv_sem=w_recv.at[index],
            device_id=device, device_id_type=MESH_ID,
        )

    act_ids = {}

    def act_copy(key, src, dst, device):
        index = act_ids.setdefault(key, len(act_ids))
        return pltpu.make_async_remote_copy(
            src_ref=src, dst_ref=dst, send_sem=a_send.at[GROUPS[key if isinstance(key, str) else key[0]]],
            recv_sem=a_recv.at[index], device_id=device, device_id_type=MESH_ID,
        )

    def drain(sem, elements):
        assert elements % wq.shape[1] == 0
        ref = wq.at[pl.ds(0, elements // wq.shape[1]), :]
        pltpu.make_async_remote_copy(
            src_ref=ref, dst_ref=ref, send_sem=sem, recv_sem=a_recv.at[0], device_id={"tp": core},
            device_id_type=MESH_ID,
        ).wait_send()

    def drain_weights(sent):
        for kind in KINDS:
            total = sum(math.prod(ref.shape) for name, ref in sent if name == kind)
            if total:
                drain(w_send.at[KINDS.index(kind)], total)

    at_z = pl.multiple_of(z * depth, depth)
    loads = {}

    def load(name, src, dst):
        copy = pltpu.make_async_copy(src, dst, load_sem.at[len(loads)])
        copy.start()
        loads[name] = copy

    load("q", w_query, wq.at[pl.ds(at_z, depth), pl.ds(0, key_cols)])
    load("k", w_key, wq.at[pl.ds(at_z, depth), pl.ds(key_cols, key_cols)])
    load("v", w_value, wq.at[pl.ds(at_z, depth), pl.ds(2 * key_cols, value_cols)])
    load("tok", tokens, tok.at[0])
    load("o0", w_mix_out.at[:, pl.ds(0, block)], wo.at[2 * z])
    load("o1", w_mix_out.at[:, pl.ds(block, block)], wo.at[2 * z + 1])
    load("shift", decay_shift, shift.at[0])
    load("g", w_gate, wg.at[pl.ds(at_z, depth), :])
    load("u", w_up, wu.at[pl.ds(at_z, depth), :])
    load("d0", w_down.at[:, pl.ds(0, block)], wd.at[2 * z])
    load("d1", w_down.at[:, pl.ds(block, block)], wd.at[2 * z + 1])
    pl.semaphore_wait(barrier, 6)
    for name in ("q", "k", "v"):
        loads[name].wait()

    tok_copy = act_copy("tok", tok.at[0], tok.at[1], {"fs": pair_z})
    shift_copy = act_copy("shift", shift_sent.at[0], shift_sent.at[1], {"fs": pair_z})

    out_units = [
        (2 * zc, None, 0, block, ()), (2 * zc + 1, None, 0, block, ()),
        (2 * zo + r, ("mid_own", zo, r), 0, block, DOWN), (2 * ze + r, ("end_a", ze, r), 0, block, DOWN),
        (2 * zf + r, ("mid_end", zf, r), 0, block, DOWN),
        (2 * ze + other_r, ("end_b", ze, other_r), 0, lane, DOWN[:2]),
        (2 * zf + other_r, ("rep_end", zf, other_r), 0, lane, DOWN[:2]),
        (2 * zo + other_r, ("rep_own", zo, other_r), 0, block, DOWN),
        (2 * ze + other_r, ("end_b", ze, other_r), lane, lane, DOWN[2:]),
        (2 * zf + other_r, ("rep_end", zf, other_r), lane, lane, DOWN[2:]),
    ]
    mixed_copy = act_copy("mixed", mixed_home, mixed_home, {"fs": pair_z})
    def home_copy(i, which):
        b, _, lo, size, _ = out_units[i]
        lanes = pl.ds(lo, size)
        src = part.at[b, chip, 1, :, lanes] if which else ffn_home.at[0, b, :, lanes]
        device = {"fs": pair_z, "tp": chip} if which else {"fs": pair_z}
        return act_copy(("home", i, which), src, ffn_home.at[which, b, :, lanes], device)

    home_near = [home_copy(i, 0) for i in range(len(out_units))]
    home_far = [home_copy(i, 1) for i in range(len(out_units))]

    @pl.when(jnp.logical_not(is_centre))
    def _():
        sent = []

        def send(name, kind, half):
            weight_copy(name, kind, z, half, {"fs": pair_z}).start()
            sent.append((kind, region(name, z, half)))

        for name in QKV:
            send(name, "end_a", r)
        loads["o0"].wait()
        loads["o1"].wait()
        send("out", "end_a", r)
        loads["tok"].wait()
        tok_copy.start()
        send(QKV[0], "end_b", other_r)
        loads["shift"].wait()
        shift_sent[0] = shift[0].astype(BF16)
        shift_copy.start()
        send("out", "end_b", other_r)
        for name in ("g", "u", "d0", "d1"):
            loads[name].wait()
        for name in ("gate0", "up0", "gate1", "up1"):
            send(name, "end_a", r)
        for name in ("gate0", "up0", "gate1", "up1"):
            send(name, "end_b", other_r)
        for name in DOWN:
            send(name, "end_a", r)
        for name in DOWN:
            send(name, "end_b", other_r)
        mixed_copy.wait_recv()
        for i, (b, _, lo, size, _) in enumerate(out_units):
            home_near[i].wait_recv()
            home_far[i].wait_recv()
            lanes = pl.ds(lo, size)
            cols = pl.ds(pl.multiple_of(b * block + lo, lane), size)
            out[:, cols] = (
                mixed_home[b, :, lanes].astype(F32)
                + ffn_home[0, b, :, lanes].astype(F32) + ffn_home[1, b, :, lanes].astype(F32)
            )
        tok_copy.wait_send()
        shift_copy.wait_send()
        drain_weights(sent)

    @pl.when(is_centre)
    def _():
        sent = []

        arrived = set()

        def incoming(name, kind, plane, half):
            if (name, kind) not in arrived:
                arrived.add((name, kind))
                weight_copy(name, kind, plane, half, {"fs": pair_z}).wait_recv()

        def send(name, kind, plane, half, device):
            weight_copy(name, kind, plane, half, device).start()
            sent.append((kind, region(name, plane, half)))

        def mid_own(*parts):
            for name in parts:
                send(name, "mid_own", z, r, {"fs": zo})

        def mid_end(*parts):
            for name in parts:
                incoming(name, "end_a", ze, r)
                send(name, "mid_end", ze, r, {"fs": zo})

        def rep_own(*parts):
            for name in parts:
                incoming(name, "mid_own", zo, r)
                send(name, "rep_own", zo, r, {"rep": other_r})

        def rep_end(*parts):
            for name in parts:
                incoming(name, "mid_end", zf, r)
                send(name, "rep_end", zf, r, {"rep": other_r})

        def rep_end_b(*parts):
            for name in parts:
                incoming(name, "end_a", ze, r)
                send(name, "end_b", ze, r, {"rep": other_r})

        def mid_own_b(*parts):
            for name in parts:
                send(name, "rep_own", z, other_r, {"fs": zo})

        def complete(*parts):
            for name in parts:
                incoming(name, "mid_own", zo, r)
                incoming(name, "end_b", ze, other_r)
                incoming(name, "rep_own", zo, other_r)
                incoming(name, "rep_end", zf, other_r)

        def norm_rows(load_rows, gain, dst, s):
            @pl.loop(0, rows // 16)
            def _(i):
                values = load_rows(pl.ds(pl.multiple_of(i * 16, 16), 16))
                scale = lax.rsqrt(jnp.mean(values * values, axis=-1, keepdims=True) + EPS)
                at = pl.multiple_of(t * rows + i * 16, 16)
                dst[s, pl.ds(at, 16), :] = (values * scale * gain[...]).astype(BF16)

        class Gather:
            def __init__(self, key, ref, s):
                def rows_of(device):
                    return ref.at[s, pl.ds(pl.multiple_of(device * rows, rows), rows), :]

                mine, theirs = rows_of(t), rows_of(chip)
                self.to_chip = act_copy((key, s, "chip"), mine, mine, {"tp": chip})
                self.to_core = act_copy((key, s, "core"), mine, mine, {"tp": core})
                self.pass_on = act_copy((key, s, "pass"), theirs, theirs, {"tp": core})
                self.from_chip = act_copy((key, s, "chip"), theirs, theirs, {"tp": chip})
                self.from_core = act_copy((key, s, "core"), rows_of(core), rows_of(core), {"tp": core})
                self.passed = act_copy((key, s, "pass"), rows_of(both), rows_of(both), {"tp": core})

            def start(self):
                self.to_chip.start()
                self.to_core.start()

            def forward(self):
                self.from_chip.wait_recv()
                self.pass_on.start()

            def finish(self):
                self.from_core.wait_recv()
                self.passed.wait_recv()

        mid_own(*QKV)
        loads["tok"].wait()
        norm_rows(lambda at: tok[0, at, :].astype(F32), mix_gain, x_mix, 0)
        mix_gather = [Gather("mix", x_mix, s) for s in range(2)]
        ffn_gather = [Gather("ffn", x_ffn, s) for s in range(2)]
        mix_gather[0].start()
        for name in ("o0", "o1", "shift", "g", "u", "d0", "d1"):
            loads[name].wait()
        bias = decay_bias[:, pl.ds(pl.multiple_of(t * key_cols, key_cols), key_cols)]
        up_cols = w_decay_up[:, pl.ds(pl.multiple_of(t * key_cols, key_cols), key_cols)]

        def project(s, lo, hi):
            @pl.loop(lo, hi)
            def _(i):
                at = pl.ds(pl.multiple_of(i * 256, 256), 256)
                x = x_mix[s, at, :]
                for n in range(0, 2 * key_cols + value_cols, 512):
                    cols = pl.ds(n, 512)
                    proj[s, at, cols] = jnp.dot(x, wq[:, cols], preferred_element_type=F32).astype(BF16)
                low = lax.dot_general(
                    x, w_decay_down[...], (((1,), (1,)), ((), ())), preferred_element_type=F32
                ).astype(BF16)
                pre = jnp.dot(low, up_cols, preferred_element_type=F32) + bias
                log_sig = jnp.minimum(pre, 0.0) - jnp.log1p(jnp.exp(-jnp.abs(pre)))
                given = shift[0, at, :] if s == 0 else shift_sent[1, at, :].astype(F32)
                shift[s, at, :] = log_sig / TAU + given

        lower = (
            lax.broadcasted_iota(jnp.int32, (BLK, BLK), 0) >= lax.broadcasted_iota(jnp.int32, (BLK, BLK), 1)
        )
        gain_cols = head_gain[:, pl.ds(pl.multiple_of(t * value_cols, value_cols), value_cols)]

        def attend(s, lo, hi):
            if lo == 0:
                state[...] = jnp.zeros_like(state)

            @pl.loop(lo, hi)
            def _(b):
                at = pl.ds(pl.multiple_of(b * BLK, BLK), BLK)
                for h in range(heads):
                    key_at = pl.ds(h * KEY_CHANNELS, KEY_CHANNELS)
                    decays = shift[s, at, key_at]
                    cumul = jnp.dot(
                        lower.astype(F32), decays, precision=lax.Precision.HIGHEST,
                        preferred_element_type=F32,
                    )
                    total = cumul[BLK - 1 :, :]
                    queries = proj[s, at, key_at].astype(F32) * KEY_CHANNELS ** (-0.5)
                    keys = proj[s, at, pl.ds(key_cols + h * KEY_CHANNELS, KEY_CHANNELS)].astype(F32)
                    values = proj[s, at, pl.ds(2 * key_cols + h * DV, DV)]
                    q_decayed = (queries * jnp.exp(cumul)).astype(BF16)
                    k_decayed = (keys * jnp.exp(-cumul)).astype(BF16)
                    weighted = (keys * jnp.exp(total - cumul)).astype(BF16)
                    scores = lax.dot_general(
                        q_decayed, k_decayed, (((1,), (1,)), ((), ())), preferred_element_type=F32
                    )
                    scores = jnp.where(lower, scores, 0.0).astype(BF16)
                    before = state[h]
                    result = jnp.dot(scores, values, preferred_element_type=F32) + lax.dot_general(
                        q_decayed, before.astype(BF16), (((1,), (1,)), ((), ())), preferred_element_type=F32
                    )
                    state[h] = jnp.exp(total) * before + lax.dot_general(
                        values, weighted, (((0,), (0,)), ((), ())), preferred_element_type=F32
                    )
                    scale = lax.rsqrt(jnp.mean(result * result, axis=-1, keepdims=True) + EPS)
                    gated[s, at, pl.ds(h * DV, DV)] = (
                        result * scale * gain_cols[:, h * DV : (h + 1) * DV]
                    ).astype(BF16)

        def mix_out(s):
            @pl.loop(0, 8)
            def _(b):
                value = jnp.dot(gated[s], wo[b], preferred_element_type=F32).astype(BF16)
                for k in range(4):
                    part[b, k, s] = value[k * rows : (k + 1) * rows]

        def reduce_copies(s):
            return (
                act_copy(("red", s, 0), part.at[:, core, s], near.at[0, s], {"tp": core}),
                act_copy(("red", s, 1), part.at[:, both, s], near.at[1, s], {"tp": core}),
                act_copy(("red", s, 2), part.at[:, chip, s], far.at[s], {"tp": chip}),
            )

        reduce = [reduce_copies(s) for s in range(2)]

        def reduce_far(s):
            reduce[s][1].wait_recv()

            @pl.loop(0, 8)
            def _(b):
                total = part[b, chip, s].astype(F32) + near[1, s, b].astype(F32)
                part[b, chip, s] = total.astype(BF16)

            reduce[s][2].start()

        def reduce_end(s):
            reduce[s][0].wait_recv()
            reduce[s][2].wait_recv()
            for b in range(8):
                cols = pl.ds(b * block, block)
                total = part[b, t, s].astype(F32) + near[0, s, b].astype(F32) + far[s, b].astype(F32)
                hid[s, :, cols] = tok[s, :, cols].astype(F32) + total
                if s == 1:
                    mixed_home[b] = total.astype(BF16)
                else:
                    out[:, cols] = total
            if s == 1:
                mixed_copy.start()
            norm_rows(lambda at: hid[s, at, :], ffn_gain, x_ffn, s)
            ffn_gather[s].start()

        def expand(s, lo, hi):
            @pl.loop(0, seq // 256)
            def _(i):
                at = pl.ds(pl.multiple_of(i * 256, 256), 256)
                x = x_ffn[s, at, :]
                for n in range(lo, hi, 256):
                    cols = pl.ds(n, min(256, hi - n))
                    gate = jnp.dot(x, wg[:, cols], preferred_element_type=F32)
                    up = jnp.dot(x, wu[:, cols], preferred_element_type=F32)
                    act[s, at, cols] = (gate / (1.0 + jnp.exp(-gate)) * up).astype(BF16)

        def piece_copies(i):
            b, _, lo, size, _ = out_units[i]
            lanes = pl.ds(lo, size)
            return (
                act_copy(("piece", i, 0), part.at[b, core, :, :, lanes], near2.at[b, 0, :, :, lanes], {"tp": core}),
                act_copy(("piece", i, 1), part.at[b, both, :, :, lanes], near2.at[b, 1, :, :, lanes], {"tp": core}),
                act_copy(("piece", i, 2), part.at[b, chip, 0, :, lanes], far2.at[b, :, lanes], {"tp": chip}),
            )

        pieces = [piece_copies(i) for i in range(len(out_units))]

        def reduce_start(s):
            reduce[s][1].start()
            reduce[s][0].start()

        def reduce_drain():
            drain(a_send.at[3], 6 * rows * width)

        begun = []

        def piece_early(i):
            b, source, lo, size, chunks = out_units[i]
            incoming(chunks[0], *source)
            for s in range(2):
                early[len(begun), s] = jnp.dot(
                    act[s, :, :down_rows], wd[b, :down_rows, lo : lo + size], preferred_element_type=F32
                )
            begun.append(i)

        def piece_dot(i):
            b, source, lo, size, chunks = out_units[i]
            for name in chunks:
                incoming(name, *source)
            lanes = pl.ds(lo, size)
            for s in range(2):
                if i in begun:
                    value = early[begun.index(i), s] + jnp.dot(
                        act[s, :, down_rows:], wd[b, down_rows:, lo : lo + size], preferred_element_type=F32
                    )
                else:
                    value = jnp.dot(act[s], wd[b, :, lo : lo + size], preferred_element_type=F32)
                value = value.astype(BF16)
                for k in range(4):
                    part[b, k, s, :, lanes] = value[k * rows : (k + 1) * rows]
            pieces[i][1].start()
            pieces[i][0].start()

        def piece_far(i):
            b, _, lo, size, _ = out_units[i]
            lanes = pl.ds(lo, size)
            pieces[i][1].wait_recv()
            for k, copy in ((1, home_far[i]), (0, pieces[i][2])):
                total = part[b, chip, k, :, lanes].astype(F32) + near2[b, 1, k, :, lanes].astype(F32)
                part[b, chip, k, :, lanes] = total.astype(BF16)
                copy.start()
            pieces[i][0].wait_recv()
            total = part[b, t, 1, :, lanes].astype(F32) + near2[b, 0, 1, :, lanes].astype(F32)
            ffn_home[0, b, :, lanes] = total.astype(BF16)
            home_near[i].start()

        def piece_end(i):
            b, _, lo, size, _ = out_units[i]
            lanes = pl.ds(lo, size)
            pieces[i][2].wait_recv()
            cols = pl.ds(pl.multiple_of(b * block + lo, lane), size)
            total = (
                part[b, t, 0, :, lanes].astype(F32) + near2[b, 0, 0, :, lanes].astype(F32)
                + far2[b, :, lanes].astype(F32)
            )
            out[:, cols] = out[:, cols] + total

        n_blk = seq // BLK
        for name in QKV:
            mid_end(name)
            rep_own(name)
        rep_end_b(*QKV[1:])
        mid_own("out")
        mix_gather[0].forward()
        mid_end("out")
        mid_own("gate0", "up0")
        rep_end(*QKV)
        rep_own("out")
        mix_gather[0].finish()
        tok_copy.wait_recv()
        norm_rows(lambda at: tok[1, at, :].astype(F32), mix_gain, x_mix, 1)
        mix_gather[1].start()
        rep_end("out")
        mid_own("gate1", "up1")
        complete(*QKV)
        project(0, 0, seq // 256)
        attend(0, 0, n_blk // 4)
        rep_own("gate0")
        attend(0, n_blk // 4, n_blk // 2)
        mix_gather[1].forward()
        attend(0, n_blk // 2, n_blk)
        complete("out")
        mix_out(0)
        reduce_start(0)
        mix_gather[1].finish()
        shift_copy.wait_recv()
        project(1, 0, seq // 512)
        reduce_far(0)
        rep_own("up0")
        project(1, seq // 512, seq // 256)
        attend(1, 0, n_blk // 2)
        mid_end("gate0")
        rep_own("gate1")
        attend(1, n_blk // 2, n_blk)
        mix_out(1)
        reduce_start(1)
        mid_end("up0")
        reduce_far(1)
        rep_own("up1")
        reduce_end(0)
        mid_end("gate1")
        rep_end("gate0")
        mid_end("up1")
        mid_own(*DOWN)
        reduce_end(1)
        rep_end("up0")
        ffn_gather[0].forward()
        rep_end("gate1")
        complete("gate0", "up0")
        ffn_gather[0].finish()
        rep_end("up1")
        expand(0, 0, cut)
        ffn_gather[1].forward()
        rep_own("down0")
        ffn_gather[1].finish()
        expand(1, 0, cut)
        rep_own("down1")
        complete("gate1", "up1")
        expand(0, cut, hidden_units)
        mid_end("down0")
        rep_own("down2")
        expand(1, cut, hidden_units)
        mid_end("down1")
        reduce_drain()
        piece_dot(0)
        piece_dot(1)
        piece_far(0)
        mid_end("down2")
        rep_end("down0")
        piece_dot(2)
        piece_far(1)
        mid_end("down3")
        mid_own_b("down3")
        piece_dot(3)
        piece_far(2)
        rep_end("down1")
        piece_far(3)
        rep_end("down2")
        piece_end(0)
        piece_end(1)
        piece_dot(5)
        rep_end("down3")
        piece_dot(4)
        piece_far(5)
        piece_dot(6)
        piece_far(4)
        piece_end(2)
        piece_end(3)
        piece_far(6)
        piece_dot(7)
        piece_early(8)
        piece_far(7)
        piece_early(9)
        piece_end(5)
        piece_dot(8)
        piece_dot(9)
        piece_far(8)
        piece_far(9)
        piece_end(4)
        piece_end(6)
        piece_end(7)
        piece_end(8)
        piece_end(9)
        for group, units in ((0, 6), (1, 6), (2, 8)):
            drain(a_send.at[group], units * rows * width)
        drain_weights(sent)


def per_device_kernel(
    tokens, mix_gain, w_query, w_key, w_value, w_decay_down, w_decay_up, decay_bias,
    decay_shift, head_gain, w_mix_out, ffn_gain, w_gate, w_up, w_down,
):
    rows, width = tokens.shape
    planes, tps = lax.axis_size("fs"), lax.axis_size("tp")
    key_cols, value_cols, hidden_units = w_query.shape[1], w_value.shape[1], w_gate.shape[1]
    depth = w_query.shape[0]
    seq = rows * tps
    blocks = 2 * planes
    block = width // blocks
    any_spec = pl.BlockSpec(memory_space=pl.ANY)
    vmem_spec = pl.BlockSpec(memory_space=pltpu.VMEM)
    large = {0, 2, 3, 4, 8, 10, 12, 13, 14}
    args = (
        tokens, mix_gain.reshape(1, -1), w_query, w_key, w_value, w_decay_down.T, w_decay_up,
        decay_bias.reshape(1, -1), decay_shift, head_gain.reshape(1, -1), w_mix_out,
        ffn_gain.reshape(1, -1), w_gate, w_up, w_down,
    )
    delta = pl.pallas_call(
        layer_kernel,
        out_shape=pltpu.VMEM((rows, width), F32),
        in_specs=[any_spec if i in large else vmem_spec for i in range(len(args))],
        out_specs=vmem_spec,
        scratch_shapes=[
            pltpu.VMEM((planes * depth, 2 * key_cols + value_cols), BF16),
            pltpu.VMEM((blocks, value_cols, block), BF16),
            pltpu.VMEM((planes * depth, hidden_units), BF16),
            pltpu.VMEM((planes * depth, hidden_units), BF16),
            pltpu.VMEM((blocks, hidden_units, block), BF16),
            pltpu.VMEM((2, rows, width), BF16),
            pltpu.VMEM((2, seq, key_cols), F32),
            pltpu.VMEM((2, seq, width), BF16),
            pltpu.VMEM((2, seq, width), BF16),
            pltpu.VMEM((2, seq, 2 * key_cols + value_cols), BF16),
            pltpu.VMEM((2, seq, value_cols), BF16),
            pltpu.VMEM((blocks, tps, 2, rows, block), BF16),
            pltpu.VMEM((2, 2, blocks, rows, block), BF16),
            pltpu.VMEM((2, blocks, rows, block), BF16),
            pltpu.VMEM((blocks, 2, 2, rows, block), BF16),
            pltpu.VMEM((blocks, rows, block), BF16),
            pltpu.VMEM((2, seq, hidden_units), BF16),
            pltpu.VMEM((2, rows, width), F32),
            pltpu.VMEM((blocks, rows, block), BF16),
            pltpu.VMEM((2, blocks, rows, block), BF16),
            pltpu.VMEM((key_cols // KEY_CHANNELS, DV, KEY_CHANNELS), F32),
            pltpu.VMEM((2, seq, key_cols), BF16),
            pltpu.VMEM((2, 2, seq, block // 2), F32),
            pltpu.SemaphoreType.DMA((11,)),
            pltpu.SemaphoreType.DMA((len(KINDS),)),
            pltpu.SemaphoreType.DMA((len(PARTS) * len(KINDS),)),
            pltpu.SemaphoreType.DMA((6,)),
            pltpu.SemaphoreType.DMA((71,)),
        ],
        compiler_params=pltpu.CompilerParams(
            collective_id=0, has_side_effects=True, vmem_limit_bytes=65000000
        ),
    )(*args)
    return tokens.astype(F32) + delta


def solution(mesh):
    shape = dict(mesh.shape)
    small = shape["rep"] == 2 and shape["fs"] == 4 and shape["tp"] == 4
    return jax.shard_map(
        per_device_kernel if small else per_device,
        mesh=mesh,
        in_specs=(
            P(("rep", "fs", "tp"), None),
            P(),
            P("fs", "tp"),
            P("fs", "tp"),
            P("fs", "tp"),
            P(),
            P(),
            P(),
            P(("rep", "fs"), "tp"),
            P(),
            P("tp", "fs"),
            P(),
            P("fs", "tp"),
            P("fs", "tp"),
            P("tp", "fs"),
        ),
        out_specs=P(("rep", "fs", "tp"), None),
        check_vma=False,
    )
```
